32 devices in a mesh: grp: 2 (over x), sp: 8 (over z, y), tp: 2 (over core).
Axes of the slice: x: 2, y: 2, z: 4, core: 2. Of those that a mesh axis runs over, the one named last changes fastest.
Arguments:
- resid: bfloat16 [2048, 2048], P(('grp', 'sp')), parts along dimension 0, may hold values from -6 to 6
- queries_first: bfloat16 [2048, 2048], P(('grp', 'sp'), 'tp'), parts along dimension 0, may hold values from -150 to 150
- keys_first: bfloat16 [2048, 2048], P(('grp', 'sp'), 'tp'), parts along dimension 0, may hold values from -6 to 6
- values_first: bfloat16 [2048, 2048], P(('grp', 'sp'), 'tp'), parts along dimension 0, may hold values from -6 to 6
- rel_first: float32 [16, 257], P('tp'), may hold values from -4 to 4
- post_first: float32 [2048], replicated, may hold values from 0.1 to 1.9
- out_first: bfloat16 [2048, 2048], P('tp', 'sp'), may hold values from -0.125 to 0.125
- pre_second: float32 [2048], replicated, may hold values from 0.1 to 1.9
- query_weight: bfloat16 [2048, 2048], P('sp', 'tp'), may hold values from -0.125 to 0.125
- key_weight: bfloat16 [2048, 2048], P('sp', 'tp'), may hold values from -0.125 to 0.125
- value_weight: bfloat16 [2048, 2048], P('sp', 'tp'), may hold values from -0.125 to 0.125
- rel_second: float32 [16, 257], P('tp'), may hold values from -4 to 4
- post_second: float32 [2048], replicated, may hold values from 0.1 to 1.9
- out_second: bfloat16 [2048, 2048], P('tp', 'sp'), may hold values from -0.125 to 0.125
Outputs:
- hidden_two: bfloat16 [2048, 2048], P(('grp', 'sp')), parts along dimension 0
The draws below stay inside these ranges and needn't reach their ends.
There are 2 independent parts, one for each index of `grp`. The reference program is written for one: setup_inputs(seed, part) draws one part's arguments, and reference() takes and returns one part's arrays. A program takes and returns all parts, laid end to end along the dimension named above; an argument that names none is the same for every part. Nothing has to cross between parts.
All inputs are finite; a program needn't handle non-finite values.
Results may differ from the reference program's by a relative error of at most 0.017.
Values may be sent and summed in bfloat16 or wider, within the bound.
A program may use at most 128 MiB of HBM per device.

```python
import jax
import jax.numpy as jnp
from jax import lax

D = 2048
HEADS = 16
SEG = 64
LEFT = 8
REACH = 512
REL_CLIP = 128
TOK_DEV = 128
TOKENS = 1024
N_SP = 8
N_TP = 2


def draw_pair(key):
    base = jax.random.fold_in(key, 41)
    key_draw = jnp.clip(jax.random.normal(jax.random.fold_in(base, 1), (TOKENS, D), jnp.float32), -6.0, 6.0)
    query_draw = jnp.clip(jax.random.normal(jax.random.fold_in(base, 2), (TOKENS, D), jnp.float32), -6.0, 6.0)
    return (query_draw, key_draw)


def draw_keys_first(key, part):
    return draw_pair(key)[1].astype(jnp.bfloat16)


def draw_queries_first(key, part):
    query_draw, key_draw = draw_pair(key)
    return query_draw.astype(jnp.bfloat16)


def block_levels(own_key, dims, cuts, smallest, top_value):
    def one(dim, parts):
        draws = jax.random.uniform(jax.random.fold_in(jax.random.fold_in(own_key, 6), dim), (parts,), jnp.float32, smallest / len(cuts), top_value / len(cuts))
        return jnp.repeat(jnp.exp(draws), dims[dim] // parts).reshape((-1,) + (1,) * (len(dims) - dim - 1))

    level = one(*cuts[0])
    for cut in cuts[1:]:
        level = level * one(*cut)
    return level


def normal_values(rng, shape, deviation, reach, shards=(), kind=jnp.bfloat16):
    values = jax.random.normal(rng, shape, jnp.float32) * deviation
    if len(shards) > 0:
        values = block_levels(rng, shape, shards, -0.22, 0.18) * values
    return jnp.clip(values, min=-reach, max=reach).astype(kind)


def setup_inputs(seed: int = 0, part: int = 0) -> dict:
    seeds = jax.random.split(jax.random.key(seed), 15)
    part_keys = jax.random.split(jax.random.fold_in(seeds[14], part), 15)
    return {
        "resid": normal_values(part_keys[0], (TOKENS, D), 1.0, 6.0, ((0, 8),)),
        "queries_first": draw_queries_first(jax.random.fold_in(jax.random.fold_in(seeds[14], part), 71), part),
        "keys_first": draw_keys_first(jax.random.fold_in(jax.random.fold_in(seeds[14], part), 71), part),
        "values_first": normal_values(part_keys[3], (TOKENS, D), 1.0, 6.0, ((0, 8), (1, 2))),
        "rel_first": normal_values(seeds[4], (HEADS, 2 * REL_CLIP + 1), 1.0, 4.0, ((0, 2),), jnp.float32),
        "post_first": jnp.clip(1.0 + 0.18 * jax.random.normal(seeds[5], (D,), jnp.float32), 0.1, 1.9),
        "out_first": normal_values(seeds[6], (D, D), D ** -0.5, 0.125, ((0, 2), (1, 8))),
        "pre_second": jnp.clip(1.0 + 0.18 * jax.random.normal(seeds[7], (D,), jnp.float32), 0.1, 1.9),
        "query_weight": normal_values(seeds[8], (D, D), D ** -0.5, 0.125, ((0, 8), (1, 2))),
        "key_weight": normal_values(seeds[9], (D, D), D ** -0.5, 0.125, ((0, 8), (1, 2))),
        "value_weight": normal_values(seeds[10], (D, D), D ** -0.5, 0.125, ((0, 8), (1, 2))),
        "rel_second": normal_values(seeds[11], (HEADS, 2 * REL_CLIP + 1), 1.0, 4.0, ((0, 2),), jnp.float32),
        "post_second": jnp.clip(1.0 + 0.18 * jax.random.normal(seeds[12], (D,), jnp.float32), 0.1, 1.9),
        "out_second": normal_values(seeds[13], (D, D), D ** -0.5, 0.125, ((0, 2), (1, 8))),
    }


EPS = 1e-06
NEG_FILL = -1e+30

def band_bias(bias_table):
    heads_here = bias_table.shape[0]
    band = (LEFT + 1) * SEG
    length = SEG + band
    index = jnp.arange(length, dtype=jnp.int32)
    distance = jnp.where(index < band, LEFT * SEG - index, LEFT * SEG + length - index)
    slot = jnp.clip(distance, -REL_CLIP, REL_CLIP) + REL_CLIP
    onehot = (slot[:, None] == jnp.arange(2 * REL_CLIP + 1, dtype=jnp.int32)[None, :]).astype(jnp.float32)
    diagonal_values = jnp.dot(bias_table, onehot.T, precision=lax.Precision.HIGHEST)
    spread = jnp.broadcast_to(diagonal_values[:, None, :], (heads_here, SEG, length)).reshape(heads_here, SEG * length)
    return spread[:, :SEG * (length - 1)].reshape(heads_here, SEG, length - 1)[:, :, :band]

def attend_band(queries, key_rows, value_rows, bias, key_live):
    rows, width = queries.shape
    heads_here = bias.shape[0]
    head_size = width // heads_here
    blocks = rows // SEG
    query_seg = queries.reshape(blocks, SEG, heads_here, head_size).astype(jnp.float32)
    key_seg = key_rows.reshape(blocks + LEFT, SEG, heads_here, head_size).astype(jnp.float32)
    value_seg = value_rows.reshape(blocks + LEFT, SEG, heads_here, head_size).astype(jnp.float32)
    live_seg = key_live.reshape(blocks + LEFT, SEG)
    key_band = jnp.concatenate([key_seg[earlier:earlier + blocks] for earlier in range(LEFT + 1)], axis=1)
    value_band = jnp.concatenate([value_seg[earlier:earlier + blocks] for earlier in range(LEFT + 1)], axis=1)
    live_band = jnp.concatenate([live_seg[earlier:earlier + blocks] for earlier in range(LEFT + 1)], axis=1)
    scores = jnp.einsum('nqhd,nkhd->nhqk', query_seg, key_band) * head_size ** (-0.5) + bias[None]
    scores = jnp.where(live_band[:, None, None, :], scores, NEG_FILL)
    largest = lax.optimization_barrier(jnp.max(scores, axis=-1, keepdims=True))
    weights = jnp.exp(scores - largest)
    weights = (weights / lax.optimization_barrier(jnp.sum(weights, axis=-1, keepdims=True))).astype(jnp.bfloat16)
    mixed = jnp.einsum('nhqk,nkhd->nqhd', weights.astype(jnp.float32), value_band)
    return mixed.astype(jnp.bfloat16).reshape(rows, width)

def attention_whole(queries, key_rows, value_rows, bias_table):
    bias = band_bias(bias_table)
    padding = jnp.zeros((REACH, key_rows.shape[1]), jnp.bfloat16)
    key_padded = jnp.concatenate([padding, key_rows], axis=0)
    value_padded = jnp.concatenate([padding, value_rows], axis=0)

    def one_block(number):
        start = (number * TOK_DEV).astype(jnp.int32)
        query_block = lax.dynamic_slice_in_dim(queries, start, TOK_DEV, 0)
        key_block = lax.dynamic_slice_in_dim(key_padded, start, TOK_DEV + REACH, 0)
        value_block = lax.dynamic_slice_in_dim(value_padded, start, TOK_DEV + REACH, 0)
        position = start - REACH + jnp.arange(TOK_DEV + REACH, dtype=jnp.int32)
        return attend_band(query_block, key_block, value_block, bias, position >= 0)
    result = lax.map(one_block, jnp.arange(N_SP, dtype=jnp.int32))
    return result.reshape(TOKENS, key_rows.shape[1])

def project_out(mixed, weight):
    width = D // N_TP
    total = jnp.zeros((mixed.shape[0], D), jnp.float32)
    for member in range(N_TP):
        term = jnp.dot(mixed[:, member * width:(member + 1) * width], weight[member * width:(member + 1) * width], preferred_element_type=jnp.float32).astype(jnp.bfloat16)
        total = total + term.astype(jnp.float32)
    return total.astype(jnp.bfloat16)

def normed(hidden, gain):
    values = hidden.astype(jnp.float32)
    scale = lax.rsqrt(lax.optimization_barrier(jnp.mean(values * values, axis=-1, keepdims=True)) + EPS)
    return (values * scale * gain).astype(jnp.bfloat16)

def residual_add(branch, residual, gain):
    values = branch.astype(jnp.float32)
    scale = lax.rsqrt(lax.optimization_barrier(jnp.mean(values * values, axis=-1, keepdims=True)) + EPS)
    return (residual.astype(jnp.float32) + values * scale * gain).astype(jnp.bfloat16)

def reference(resid, queries_first, keys_first, values_first, rel_first, post_first, out_first, pre_second, query_weight, key_weight, value_weight, rel_second, post_second, out_second):
    first = attention_whole(queries_first, keys_first, values_first, rel_first)
    hidden_one = residual_add(project_out(first, out_first), resid, post_first)
    inputs_two = normed(hidden_one, pre_second)
    queries_two = jnp.dot(inputs_two, query_weight, preferred_element_type=jnp.float32).astype(jnp.bfloat16)
    keys_two = jnp.dot(inputs_two, key_weight, preferred_element_type=jnp.float32).astype(jnp.bfloat16)
    values_two = jnp.dot(inputs_two, value_weight, preferred_element_type=jnp.float32).astype(jnp.bfloat16)
    second = attention_whole(queries_two, keys_two, values_two, rel_second)
    return residual_add(project_out(second, out_second), hidden_one, post_second)
```

```python
import jax
import jax.numpy as jnp
from jax import lax
from jax.experimental import pallas as pl
from jax.experimental.pallas import tpu as pltpu
from jax.sharding import PartitionSpec as P

MESH = pl.DeviceIdType.MESH
BF16 = jnp.bfloat16
F32 = jnp.float32

SEG = 64
LEFT = 8
REACH = 512
REL_CLIP = 128


EPS = 1e-06
NEG_FILL = -1e30


def from_behind(value, axis, steps):
    count = lax.axis_size(axis)
    initial, last = (max(0, -steps), min(count, count - steps))
    return lax.ppermute(value, axis, [(source, source + steps) for source in range(initial, last)])


def band_bias(bias_table):
    heads_here = bias_table.shape[0]
    band = (LEFT + 1) * SEG
    length = SEG + band
    index = jnp.arange(length, dtype=jnp.int32)
    distance = jnp.where(index < band, LEFT * SEG - index, LEFT * SEG + length - index)
    slot = jnp.clip(distance, -REL_CLIP, REL_CLIP) + REL_CLIP
    onehot = (slot[:, None] == jnp.arange(2 * REL_CLIP + 1, dtype=jnp.int32)[None, :]).astype(
        jnp.float32
    )
    diagonal_values = jnp.dot(bias_table, onehot.T, precision=lax.Precision.HIGHEST)
    spread = jnp.broadcast_to(diagonal_values[:, None, :], (heads_here, SEG, length)).reshape(
        heads_here, SEG * length
    )
    return spread[:, : SEG * (length - 1)].reshape(heads_here, SEG, length - 1)[:, :, :band]


def attend_band(queries, key_rows, value_rows, bias, key_live):
    rows, width = queries.shape
    heads_here = bias.shape[0]
    head_size = width // heads_here
    blocks = rows // SEG
    query_seg = queries.reshape(blocks, SEG, heads_here, head_size)
    key_seg = key_rows.reshape(blocks + LEFT, SEG, heads_here, head_size)
    value_seg = value_rows.reshape(blocks + LEFT, SEG, heads_here, head_size)
    live_seg = key_live.reshape(blocks + LEFT, SEG)
    key_band = jnp.concatenate(
        [key_seg[earlier : earlier + blocks] for earlier in range(LEFT + 1)], axis=1
    )
    value_band = jnp.concatenate(
        [value_seg[earlier : earlier + blocks] for earlier in range(LEFT + 1)], axis=1
    )
    live_band = jnp.concatenate(
        [live_seg[earlier : earlier + blocks] for earlier in range(LEFT + 1)], axis=1
    )
    scores = jnp.einsum("nqhd,nkhd->nhqk", query_seg, key_band, preferred_element_type=jnp.float32)
    scores = scores * head_size ** (-0.5) + bias[None]
    scores = jnp.where(live_band[:, None, None, :], scores, NEG_FILL)
    largest = jnp.max(scores, axis=-1, keepdims=True)
    weights = jnp.exp(scores - largest)
    weights = (weights / jnp.sum(weights, axis=-1, keepdims=True)).astype(jnp.bfloat16)
    mixed = jnp.einsum("nhqk,nkhd->nqhd", weights, value_band, preferred_element_type=jnp.float32)
    return mixed.astype(jnp.bfloat16).reshape(rows, width)


def extend_rows(pieces, member, own_rows):
    joined = jnp.concatenate([piece[member] for piece in pieces] + [own_rows], axis=0)
    return joined


def normed(hidden, gain):
    values = hidden.astype(jnp.float32)
    scale = lax.rsqrt(jnp.mean(values * values, axis=-1, keepdims=True) + EPS)
    return (values * scale * gain).astype(jnp.bfloat16)


def residual_add(branch, residual, gain):
    values = branch.astype(jnp.float32)
    scale = lax.rsqrt(jnp.mean(values * values, axis=-1, keepdims=True) + EPS)
    return (residual.astype(jnp.float32) + values * scale * gain).astype(jnp.bfloat16)


def combine(mixed, weight, residual, gain):
    partial_rows = jnp.dot(
        mixed, lax.all_gather(weight, "sp", axis=1, tiled=True), preferred_element_type=jnp.float32
    )
    branch = lax.psum_scatter(
        partial_rows.astype(jnp.bfloat16), "tp", scatter_dimension=0, tiled=True
    )
    return residual_add(branch, residual, gain)


def full_rows(share):
    return lax.all_gather(share, "tp", axis=0, tiled=True)


def shards(
    resid,
    queries_first,
    keys_first,
    values_first,
    rel_first,
    post_first,
    out_first,
    pre_second,
    query_weight,
    key_weight,
    value_weight,
    rel_second,
    post_second,
    out_second,
):
    tok_rows = resid.shape[0]
    n_sp = lax.axis_size("sp")
    if (
        rel_first.shape[0] == n_sp
        and n_sp % 2 == 0
        and lax.axis_size("tp") == 2
        and lax.axis_size("grp") == 2
        and REACH % tok_rows == 0
        and tok_rows == REL_CLIP
    ):
        return by_heads(
            resid, queries_first, keys_first, values_first, rel_first, post_first, out_first,
            pre_second, query_weight, key_weight, value_weight, rel_second, post_second, out_second,
        )
    depth = (REACH + tok_rows - 1) // tok_rows
    anchor = lax.axis_index("sp") * tok_rows
    key_live = anchor - REACH + jnp.arange(tok_rows + REACH, dtype=jnp.int32) >= 0
    share_rows = tok_rows // lax.axis_size("tp")
    base_rows = lax.dynamic_slice_in_dim(resid, lax.axis_index("tp") * share_rows, share_rows, 0)
    earlier_first = [
        from_behind((keys_first, values_first), "sp", distance) for distance in range(depth, 0, -1)
    ]
    key_ext = extend_rows(earlier_first, 0, keys_first)
    value_ext = extend_rows(earlier_first, 1, values_first)
    first = attend_band(queries_first, key_ext, value_ext, band_bias(rel_first), key_live)
    hidden_one = combine(first, out_first, base_rows, post_first)
    inputs_two = full_rows(normed(hidden_one, pre_second))
    query_sum = jnp.dot(
        inputs_two,
        lax.all_gather(query_weight, "sp", axis=0, tiled=True),
        preferred_element_type=jnp.float32,
    )
    key_sum = jnp.dot(
        inputs_two,
        lax.all_gather(key_weight, "sp", axis=0, tiled=True),
        preferred_element_type=jnp.float32,
    )
    value_sum = jnp.dot(
        inputs_two,
        lax.all_gather(value_weight, "sp", axis=0, tiled=True),
        preferred_element_type=jnp.float32,
    )
    queries_two = query_sum.astype(jnp.bfloat16)
    keys_two = key_sum.astype(jnp.bfloat16)
    values_two = value_sum.astype(jnp.bfloat16)
    earlier_second = [
        from_behind((keys_two, values_two), "sp", distance) for distance in range(depth, 0, -1)
    ]
    key_ext_two = extend_rows(earlier_second, 0, keys_two)
    value_ext_two = extend_rows(earlier_second, 1, values_two)
    second = attend_band(queries_two, key_ext_two, value_ext_two, band_bias(rel_second), key_live)
    hidden_two = combine(second, out_second, hidden_one, post_second)
    return full_rows(hidden_two)


def scaled(values):
    return values * lax.rsqrt(jnp.mean(values * values, axis=-1, keepdims=True) + EPS)


def build_kernel(n, tok, head, width, reach):
    share = tok // 2
    cols = width // n
    span = reach + tok
    levels = n // 2
    depth = n * head
    dhalf = depth // 2
    wrows = width // n
    hrows = wrows // 2
    pieces = 4
    wide = width // pieces

    def kernel(
        q_hbm, k_hbm, v_hbm, wq_hbm, wk_hbm, wv_hbm, resid_hbm, o1_hbm, o2_hbm,
        rel1, rel2, post1, pre2, post2,
        out_ref,
        heads, weights, outs, res, bias, own_mix, mixed, parts, inbox, joined, branch, rows2, last,
        loc_sem, hs, hr, ws, wr, wf, mzs, mzr, mys, myr, ozs, ozr, oxs, oxr,
        ps, pr, bs, br, rzs, rzr, rys, ryr, rds, rdr, fs, fr,
    ):
        s = lax.axis_index("sp")
        t = lax.axis_index("tp")
        g = lax.axis_index("grp")
        u = 1 - t
        z = s // 2
        y = lax.rem(s, 2)
        v = 1 - y
        side = 2 * z + v
        turn = 1 - 2 * lax.rem(z, 2)

        def rcopy(src, dst, ssem, rsem, sp, tp, grp=g):
            return pltpu.make_async_remote_copy(
                src_ref=src, dst_ref=dst, send_sem=ssem, recv_sem=rsem,
                device_id={"grp": grp, "sp": sp, "tp": tp}, device_id_type=MESH,
            )

        def peer(k):
            return lax.rem(s + k, n)

        def near_level(i):
            return lax.rem(z + turn * i + levels, levels)

        def arrived(ref, sem):
            pltpu.make_async_copy(ref, ref, sem).wait()

        barrier = pltpu.get_barrier_semaphore()
        for k in range(1, n):
            pl.semaphore_signal(
                barrier, inc=1, device_id={"grp": g, "sp": peer(k), "tp": t}, device_id_type=MESH
            )
        pl.semaphore_signal(
            barrier, inc=1, device_id={"grp": g, "sp": s, "tp": u}, device_id_type=MESH
        )
        pl.semaphore_signal(
            barrier, inc=1, device_id={"grp": 1 - g, "sp": s, "tp": t}, device_id_type=MESH
        )
        pl.semaphore_wait(barrier, n + 1)

        def lanes(j):
            return pl.ds(pl.multiple_of(j * head, head), head)

        def trows(j, base=0):
            return pl.ds(pl.multiple_of(base + j * tok, tok), tok)

        qkv = (q_hbm, k_hbm, v_hbm)
        wqkv = (wq_hbm, wk_hbm, wv_hbm)
        out_hbm = (o1_hbm, o2_hbm)

        def head_copy(i, j):
            dst = heads.at[i, trows(s, reach)]
            return rcopy(qkv[i].at[:, lanes(j)], dst, hs, hr.at[s], j, t)

        def weight_half(src, part):
            start = pl.multiple_of(src * wrows + part * hrows, hrows)
            return weights.at[pl.ds(start, hrows)]

        def weight_copy(i, j):
            start = pl.multiple_of(s * wrows + g * hrows, hrows)
            piece = wqkv[i].at[pl.ds(pl.multiple_of(g * hrows, hrows), hrows), lanes(j)]
            dst = weights.at[pl.ds(start, hrows), pl.ds(i * head, head)]
            return rcopy(piece, dst, ws, wr.at[s, g], j, t)

        def weight_hand(src):
            piece = weight_half(src, g)
            return rcopy(piece, piece, wf, wr.at[src, g], s, t, 1 - g)

        def out_half(layer, c, part):
            return outs.at[layer, c, pl.ds(pl.multiple_of(part * dhalf, dhalf), dhalf)]

        def out_own(layer, to):
            piece = out_hbm[layer].at[pl.ds(pl.multiple_of(g * dhalf, dhalf), dhalf)]
            return rcopy(
                piece, out_half(layer, z, g), ozs.at[layer], ozr.at[layer, z], 2 * to + y, t
            )

        def out_pass(layer, c, to):
            piece = out_half(layer, c, g)
            return rcopy(piece, piece, ozs.at[layer], ozr.at[layer, c], 2 * to + y, t)

        def out_hand(layer, c):
            piece = out_half(layer, c, g)
            return rcopy(piece, piece, oxs.at[layer], oxr.at[layer, c], s, t, 1 - g)

        def out_start(layer):
            @pl.when(z < levels - 1)
            def _():
                out_own(layer, z + 1).start()

            @pl.when(z > 0)
            def _():
                out_own(layer, z - 1).start()

        def out_hop(layer, d):
            @pl.when(z >= d)
            def _():
                arrived(out_half(layer, z - d, g), ozr.at[layer, z - d])

                @pl.when(z < levels - 1)
                def _():
                    out_pass(layer, z - d, z + 1).start()

                out_hand(layer, z - d).start()

            @pl.when(z + d < levels)
            def _():
                arrived(out_half(layer, z + d, g), ozr.at[layer, z + d])

                @pl.when(z > 0)
                def _():
                    out_pass(layer, z + d, z - 1).start()

                out_hand(layer, z + d).start()

        def out_drain(layer):
            for at in range(levels):
                count = (1 + at if at < levels - 1 else 0) + (levels - at if at > 0 else 0)
                block = rows2.at[pl.ds(0, count)]

                @pl.when(z == at)
                def _():
                    arrived(block, ozs.at[layer])

            arrived(rows2.at[pl.ds(0, levels - 1)], oxs.at[layer])

        out_start(0)
        for k in range(1, n):
            for i in range(3):
                head_copy(i, peer(k)).start()
        for i in range(3):
            pltpu.make_async_copy(
                qkv[i].at[:, lanes(s)], heads.at[i, trows(s, reach)], hr.at[s]
            ).start()
        for i in range(3):
            pltpu.make_async_copy(
                wqkv[i].at[:, lanes(s)],
                weights.at[pl.ds(pl.multiple_of(s * wrows, wrows), wrows), pl.ds(i * head, head)],
                wr.at[s, 0],
            ).start()
        local = [
            pltpu.make_async_copy(o1_hbm, outs.at[0, z], loc_sem.at[0]),
            pltpu.make_async_copy(o2_hbm, outs.at[1, z], loc_sem.at[1]),
            pltpu.make_async_copy(
                resid_hbm.at[pl.ds(pl.multiple_of(t * share, share), share)], res, loc_sem.at[2]
            ),
        ]
        for copy in local:
            copy.start()

        near = 2 * REL_CLIP
        query = lax.broadcasted_iota(jnp.int32, (tok, span), 0) // SEG
        key = lax.broadcasted_iota(jnp.int32, (tok, span), 1) // SEG
        live = (key >= query) & (key <= query + LEFT)
        for layer, rel in enumerate((rel1, rel2)):
            table = rel[pl.ds(s, 1), :]
            top = table[:, near : near + 1]
            entry = lax.broadcasted_iota(jnp.int32, (near, near + tok), 0)
            place = lax.broadcasted_iota(jnp.int32, (near, near + tok), 1)
            flip = (entry + place == near).astype(F32)
            line = jnp.dot(
                jnp.broadcast_to(table[:, :near], (8, near)), flip,
                preferred_element_type=F32, precision=lax.Precision.HIGHEST,
            )[:1]
            spot = lax.broadcasted_iota(jnp.int32, line.shape, 1)
            line = jnp.where((spot == 0) | (spot >= near), top, line)
            spread = jnp.broadcast_to(line, (tok, near + tok))
            row = lax.broadcasted_iota(jnp.int32, spread.shape, 0)
            step = 1
            while step < tok:
                moved = pltpu.roll(spread, step, 1)
                spread = jnp.where(lax.rem(row // step, 2) == 1, moved, spread)
                step *= 2
            far = jnp.broadcast_to(top, (tok, span - near))
            whole = jnp.concatenate([far, spread[:, :near]], axis=1)
            bias[layer] = jnp.where(live, whole, NEG_FILL)

        heads[1, :reach] = jnp.zeros((reach, head), BF16)
        heads[2, :reach] = jnp.zeros((reach, head), BF16)

        def attend(layer, b):
            qb = heads[0, trows(b, reach)]
            kb = heads[1, pl.ds(pl.multiple_of(b * tok, tok), span)]
            vb = heads[2, pl.ds(pl.multiple_of(b * tok, tok), span)]
            scores = lax.dot_general(
                qb, kb, (((1,), (1,)), ((), ())), preferred_element_type=F32
            ) * head ** (-0.5) + bias[layer]
            column = lax.broadcasted_iota(jnp.int32, scores.shape, 1)
            scores = jnp.where(column >= reach - b * tok, scores, NEG_FILL)
            e = jnp.exp(scores - jnp.max(scores, axis=-1, keepdims=True))
            e = (e * (1.0 / jnp.sum(e, axis=-1, keepdims=True))).astype(BF16)
            return jnp.dot(e, vb, preferred_element_type=F32).astype(BF16)

        def mix_z(layer, b):
            dst = mixed.at[layer, s, trows(lax.rem(b, 2))]
            return rcopy(
                own_mix.at[layer, b], dst, mzs.at[layer], mzr.at[layer, z], 2 * (b // 2) + y, t
            )

        def mix_y(layer, c):
            block = mixed.at[layer, 2 * c + y]
            return rcopy(block, block, mys.at[layer], myr.at[layer, c], side, t)

        def run_heads(layer, order, wait_block):
            def one(i, _):
                b = order(i)
                wait_block(b)
                result = attend(layer, b)

                @pl.when(b // 2 != z)
                def _():
                    own_mix[layer, b] = result
                    mix_z(layer, b).start()

                @pl.when(b // 2 == z)
                def _():
                    mixed[layer, s, trows(lax.rem(b, 2))] = result

                    @pl.when(lax.rem(b, 2) == 1)
                    def _():
                        mix_y(layer, z).start()

                return 0

            lax.fori_loop(0, n, one, 0)

        def forward_mix(layer):
            def one(i, _):
                c = near_level(i)
                arrived(mixed.at[layer, 2 * c + y], mzr.at[layer, c])
                mix_y(layer, c).start()
                return 0

            lax.fori_loop(1, levels, one, 0)

        def pcopy(layer, c):
            return rcopy(
                parts.at[layer, c, u], inbox.at[layer, c],
                ps.at[layer], pr.at[layer, c], s, u,
            )

        def bcopy(layer, c):
            return rcopy(
                joined.at[layer, c, v], branch.at[layer, y, c], bs.at[layer], br.at[layer], side, t
            )

        def project_branch(layer):
            for c in range(levels):
                arrived(mixed.at[layer, 2 * c + v], myr.at[layer, c])
            local[layer].wait()

            def project(c):
                @pl.when(c != z)
                def _():
                    arrived(out_half(layer, c, 1 - g), oxr.at[layer, c])

                lhs = jnp.concatenate([mixed[layer, j] for j in range(n)], axis=1)
                part = jnp.dot(lhs, outs[layer, c], preferred_element_type=F32).astype(BF16)
                for p in range(2):
                    for q in range(2):
                        parts[layer, c, q, p] = part[p * tok + q * share : p * tok + (q + 1) * share]
                pcopy(layer, c).start()

            def join(c):
                arrived(inbox.at[layer, c], pr.at[layer, c])
                both = parts[layer, c, t].astype(F32) + inbox[layer, c].astype(F32)
                joined[layer, c] = both.astype(BF16)
                bcopy(layer, c).start()
                branch[layer, y, c] = joined[layer, c, y]

            def step(i, _):
                project(near_level(i))

                @pl.when(i > 0)
                def _():
                    join(near_level(i - 1))

                return 0

            lax.fori_loop(0, levels, step, 0)
            join(near_level(levels - 1))
            arrived(branch.at[layer, v], br.at[layer])
            values = jnp.concatenate(
                [branch[layer, j % 2, j // 2] for j in range(n)], axis=1
            )
            return values.astype(F32)

        def branch_drain(layer):
            arrived(own_mix.at[layer, pl.ds(0, n - 2)], mzs.at[layer])
            arrived(mixed.at[layer, pl.ds(0, levels)], mys.at[layer])
            arrived(inbox.at[layer], ps.at[layer])
            arrived(branch.at[layer, 0], bs.at[layer])

        def heads_ready(b):
            arrived(heads.at[:, trows(b, reach)], hr.at[b])

        out_hop(0, 1)
        run_heads(0, lambda i: i, heads_ready)
        out_hop(0, 2)
        forward_mix(0)
        for k in range(1, n):
            for i in range(3):
                weight_copy(i, peer(k)).start()
        for d in range(3, levels):
            out_hop(0, d)
        values = project_branch(0)
        local[2].wait()
        hidden = (res[...].astype(F32) + scaled(values) * post1[...]).astype(BF16)
        res[...] = hidden
        rows2[2 * s + t] = (scaled(hidden.astype(F32)) * pre2[...]).astype(BF16)

        def piece_of(item, m):
            return rows2.at[item, :, pl.ds(pl.multiple_of(m * wide, wide), wide)]

        def row_z(c, m, to):
            block = piece_of(2 * (2 * c + y) + t, m)
            return rcopy(block, block, rzs, rzr.at[c, m], 2 * to + y, t)

        def row_y(c, m):
            block = piece_of(2 * (2 * c + y) + t, m)
            return rcopy(block, block, rys, ryr.at[c, m], side, t)

        def row_d(src, m):
            block = piece_of(2 * src + t, m)
            return rcopy(block, block, rds, rdr.at[src], s, u)

        def own_rows(m, _):
            @pl.when(z < levels - 1)
            def _():
                row_z(z, m, z + 1).start()

            @pl.when(z > 0)
            def _():
                row_z(z, m, z - 1).start()

            row_y(z, m).start()
            row_d(s, m).start()
            return 0

        lax.fori_loop(0, pieces, own_rows, 0)

        def hand_weights(k, _):
            src = peer(k)
            arrived(weight_half(src, g), wr.at[src, g])
            weight_hand(src).start()
            return 0

        lax.fori_loop(1, n, hand_weights, 0)

        def from_level(c, m, on, to):
            arrived(piece_of(2 * (2 * c + y) + t, m), rzr.at[c, m])

            @pl.when(on)
            def _():
                row_z(c, m, to).start()

            row_y(c, m).start()
            row_d(2 * c + y, m).start()

        def from_side(c, m):
            arrived(piece_of(2 * (2 * c + v) + t, m), ryr.at[c, m])
            row_d(2 * c + v, m).start()

        def rows_hop(d):
            def one(m, _):
                if d < levels:
                    @pl.when(z >= d)
                    def _():
                        from_level(z - d, m, z < levels - 1, z + 1)

                    @pl.when(z + d < levels)
                    def _():
                        from_level(z + d, m, z > 0, z - 1)

                if d == 1:
                    from_side(z, m)
                else:
                    @pl.when(z >= d - 1)
                    def _():
                        from_side(z - (d - 1), m)

                    @pl.when(z + d - 1 < levels)
                    def _():
                        from_side(z + (d - 1), m)

                return 0

            lax.fori_loop(0, pieces, one, 0)

        for d in range(1, levels + 1):
            rows_hop(d)
            if d == 1:
                out_start(1)
        out_hop(1, 1)

        def weights_ready(k, _):
            src = peer(k)
            arrived(weight_half(src, 1 - g), wr.at[src, 1 - g])
            return 0

        lax.fori_loop(1, n, weights_ready, 0)
        arrived(weights.at[pl.ds(pl.multiple_of(s * wrows, wrows), wrows)], wr.at[s, 0])

        def project_rows(i, _):
            c = near_level(i)
            arrived(rows2.at[4 * c + u], rdr.at[2 * c])
            arrived(rows2.at[4 * c + 2 + u], rdr.at[2 * c + 1])
            lhs = rows2[pl.ds(4 * c, 4)].reshape(2 * tok, width)
            both = jnp.dot(lhs, weights[...], preferred_element_type=F32).astype(BF16)
            start = pl.ds(pl.multiple_of(reach + c * 2 * tok, tok), 2 * tok)
            for i in range(3):
                heads[i, start] = both[:, i * head : (i + 1) * head]
            return 0

        lax.fori_loop(0, levels, project_rows, 0)
        for d in range(2, levels - 1):
            out_hop(1, d)
        run_heads(1, lambda i: lax.rem(2 * z + 2 + i, n), lambda b: None)
        forward_mix(1)
        if levels > 2:
            out_hop(1, levels - 1)
        values = project_branch(1)
        done = (res[...].astype(F32) + scaled(values) * post2[...]).astype(BF16)
        last[t] = done
        final = rcopy(last.at[t], last.at[t], fs, fr, s, u)
        final.start()

        arrived(heads.at[:, pl.ds(reach, (n - 1) * tok)], hs)
        arrived(weights.at[pl.ds(0, (n - 1) * hrows)], ws)
        arrived(weights.at[pl.ds(0, (n - 1) * hrows)], wf)
        for layer in range(2):
            out_drain(layer)
            branch_drain(layer)
        for at in range(levels):
            count = (1 + at if at < levels - 1 else 0) + (levels - at if at > 0 else 0)
            block = rows2.at[pl.ds(0, count)]

            @pl.when(z == at)
            def _():
                arrived(block, rzs)

        arrived(rows2.at[pl.ds(0, levels)], rys)
        arrived(rows2.at[pl.ds(0, n)], rds)
        final.wait_send()
        rcopy(last.at[u], last.at[u], fs, fr, s, u).wait_recv()
        out_ref[:share] = last[0]
        out_ref[share:] = last[1]

    dma = pltpu.SemaphoreType.DMA
    scratch = [
        pltpu.VMEM((3, reach + n * tok, head), BF16),
        pltpu.VMEM((width, 3 * head), BF16),
        pltpu.VMEM((2, levels, depth, cols), BF16),
        pltpu.VMEM((share, width), BF16),
        pltpu.VMEM((2, tok, span), F32),
        pltpu.VMEM((2, n, tok, head), BF16),
        pltpu.VMEM((2, n, 2 * tok, head), BF16),
        pltpu.VMEM((2, levels, 2, 2, share, cols), BF16),
        pltpu.VMEM((2, levels, 2, share, cols), BF16),
        pltpu.VMEM((2, levels, 2, share, cols), BF16),
        pltpu.VMEM((2, 2, levels, share, cols), BF16),
        pltpu.VMEM((2 * n, share, width), BF16),
        pltpu.VMEM((2, share, width), BF16),
        dma((3,)),
        dma, dma((n,)),
        dma, dma((n, 2)), dma,
        dma((2,)), dma((2, levels)), dma((2,)), dma((2, levels)),
        dma((2,)), dma((2, levels)), dma((2,)), dma((2, levels)),
        dma((2,)), dma((2, levels)), dma((2,)), dma((2,)),
        dma, dma((levels, pieces)), dma, dma((levels, pieces)), dma, dma((n,)),
        dma, dma,
    ]
    return kernel, scratch


def by_heads(
    resid, queries_first, keys_first, values_first, rel_first, post_first, out_first, pre_second,
    query_weight, key_weight, value_weight, rel_second, post_second, out_second,
):
    n = lax.axis_size("sp")
    tok, width = resid.shape
    head = queries_first.shape[1] // rel_first.shape[0]
    kernel, scratch = build_kernel(n, tok, head, width, REACH)
    hbm = pl.BlockSpec(memory_space=pltpu.HBM)
    vmem = pl.BlockSpec(memory_space=pltpu.VMEM)
    return pl.pallas_call(
        kernel,
        out_shape=jax.ShapeDtypeStruct((tok, width), BF16),
        in_specs=[hbm] * 9 + [vmem] * 5,
        out_specs=vmem,
        scratch_shapes=scratch,
        compiler_params=pltpu.CompilerParams(
            collective_id=0, has_side_effects=True, vmem_limit_bytes=60 * 2**20
        ),
    )(
        queries_first, keys_first, values_first, query_weight, key_weight, value_weight, resid,
        out_first, out_second, rel_first, rel_second,
        post_first[None], pre_second[None], post_second[None],
    )


def solution(mesh):
    in_specs = (
        P(("grp", "sp"), None),
        P(("grp", "sp"), "tp"),
        P(("grp", "sp"), "tp"),
        P(("grp", "sp"), "tp"),
        P("tp", None),
        P(),
        P("tp", "sp"),
        P(),
        P("sp", "tp"),
        P("sp", "tp"),
        P("sp", "tp"),
        P("tp", None),
        P(),
        P("tp", "sp"),
    )
    out_specs = P(("grp", "sp"), None)
    return jax.shard_map(shards, mesh=mesh, in_specs=in_specs, out_specs=out_specs, check_vma=False)
```

```python
import jax
import jax.numpy as jnp
from jax import lax
from jax.experimental import pallas as pl
from jax.experimental.pallas import tpu as pltpu
from jax.sharding import PartitionSpec as P

MESH = pl.DeviceIdType.MESH
BF16 = jnp.bfloat16
F32 = jnp.float32

SEG = 64
LEFT = 8
REACH = 512
REL_CLIP = 128


EPS = 1e-06
NEG_FILL = -1e30


def from_behind(value, axis, steps):
    count = lax.axis_size(axis)
    initial, last = (max(0, -steps), min(count, count - steps))
    return lax.ppermute(value, axis, [(source, source + steps) for source in range(initial, last)])


def band_bias(bias_table):
    heads_here = bias_table.shape[0]
    band = (LEFT + 1) * SEG
    length = SEG + band
    index = jnp.arange(length, dtype=jnp.int32)
    distance = jnp.where(index < band, LEFT * SEG - index, LEFT * SEG + length - index)
    slot = jnp.clip(distance, -REL_CLIP, REL_CLIP) + REL_CLIP
    onehot = (slot[:, None] == jnp.arange(2 * REL_CLIP + 1, dtype=jnp.int32)[None, :]).astype(
        jnp.float32
    )
    diagonal_values = jnp.dot(bias_table, onehot.T, precision=lax.Precision.HIGHEST)
    spread = jnp.broadcast_to(diagonal_values[:, None, :], (heads_here, SEG, length)).reshape(
        heads_here, SEG * length
    )
    return spread[:, : SEG * (length - 1)].reshape(heads_here, SEG, length - 1)[:, :, :band]


def attend_band(queries, key_rows, value_rows, bias, key_live):
    rows, width = queries.shape
    heads_here = bias.shape[0]
    head_size = width // heads_here
    blocks = rows // SEG
    query_seg = queries.reshape(blocks, SEG, heads_here, head_size)
    key_seg = key_rows.reshape(blocks + LEFT, SEG, heads_here, head_size)
    value_seg = value_rows.reshape(blocks + LEFT, SEG, heads_here, head_size)
    live_seg = key_live.reshape(blocks + LEFT, SEG)
    key_band = jnp.concatenate(
        [key_seg[earlier : earlier + blocks] for earlier in range(LEFT + 1)], axis=1
    )
    value_band = jnp.concatenate(
        [value_seg[earlier : earlier + blocks] for earlier in range(LEFT + 1)], axis=1
    )
    live_band = jnp.concatenate(
        [live_seg[earlier : earlier + blocks] for earlier in range(LEFT + 1)], axis=1
    )
    scores = jnp.einsum("nqhd,nkhd->nhqk", query_seg, key_band, preferred_element_type=jnp.float32)
    scores = scores * head_size ** (-0.5) + bias[None]
    scores = jnp.where(live_band[:, None, None, :], scores, NEG_FILL)
    largest = jnp.max(scores, axis=-1, keepdims=True)
    weights = jnp.exp(scores - largest)
    weights = (weights / jnp.sum(weights, axis=-1, keepdims=True)).astype(jnp.bfloat16)
    mixed = jnp.einsum("nhqk,nkhd->nqhd", weights, value_band, preferred_element_type=jnp.float32)
    return mixed.astype(jnp.bfloat16).reshape(rows, width)


def extend_rows(pieces, member, own_rows):
    joined = jnp.concatenate([piece[member] for piece in pieces] + [own_rows], axis=0)
    return joined


def normed(hidden, gain):
    values = hidden.astype(jnp.float32)
    scale = lax.rsqrt(jnp.mean(values * values, axis=-1, keepdims=True) + EPS)
    return (values * scale * gain).astype(jnp.bfloat16)


def residual_add(branch, residual, gain):
    values = branch.astype(jnp.float32)
    scale = lax.rsqrt(jnp.mean(values * values, axis=-1, keepdims=True) + EPS)
    return (residual.astype(jnp.float32) + values * scale * gain).astype(jnp.bfloat16)


def combine(mixed, weight, residual, gain):
    partial_rows = jnp.dot(
        mixed, lax.all_gather(weight, "sp", axis=1, tiled=True), preferred_element_type=jnp.float32
    )
    branch = lax.psum_scatter(
        partial_rows.astype(jnp.bfloat16), "tp", scatter_dimension=0, tiled=True
    )
    return residual_add(branch, residual, gain)


def full_rows(share):
    return lax.all_gather(share, "tp", axis=0, tiled=True)


def shards(
    resid,
    queries_first,
    keys_first,
    values_first,
    rel_first,
    post_first,
    out_first,
    pre_second,
    query_weight,
    key_weight,
    value_weight,
    rel_second,
    post_second,
    out_second,
):
    tok_rows = resid.shape[0]
    n_sp = lax.axis_size("sp")
    if (
        rel_first.shape[0] == n_sp
        and n_sp % 2 == 0
        and lax.axis_size("tp") == 2
        and lax.axis_size("grp") == 2
        and REACH % tok_rows == 0
        and tok_rows == REL_CLIP
    ):
        return by_heads(
            resid, queries_first, keys_first, values_first, rel_first, post_first, out_first,
            pre_second, query_weight, key_weight, value_weight, rel_second, post_second, out_second,
        )
    depth = (REACH + tok_rows - 1) // tok_rows
    anchor = lax.axis_index("sp") * tok_rows
    key_live = anchor - REACH + jnp.arange(tok_rows + REACH, dtype=jnp.int32) >= 0
    share_rows = tok_rows // lax.axis_size("tp")
    base_rows = lax.dynamic_slice_in_dim(resid, lax.axis_index("tp") * share_rows, share_rows, 0)
    earlier_first = [
        from_behind((keys_first, values_first), "sp", distance) for distance in range(depth, 0, -1)
    ]
    key_ext = extend_rows(earlier_first, 0, keys_first)
    value_ext = extend_rows(earlier_first, 1, values_first)
    first = attend_band(queries_first, key_ext, value_ext, band_bias(rel_first), key_live)
    hidden_one = combine(first, out_first, base_rows, post_first)
    inputs_two = full_rows(normed(hidden_one, pre_second))
    query_sum = jnp.dot(
        inputs_two,
        lax.all_gather(query_weight, "sp", axis=0, tiled=True),
        preferred_element_type=jnp.float32,
    )
    key_sum = jnp.dot(
        inputs_two,
        lax.all_gather(key_weight, "sp", axis=0, tiled=True),
        preferred_element_type=jnp.float32,
    )
    value_sum = jnp.dot(
        inputs_two,
        lax.all_gather(value_weight, "sp", axis=0, tiled=True),
        preferred_element_type=jnp.float32,
    )
    queries_two = query_sum.astype(jnp.bfloat16)
    keys_two = key_sum.astype(jnp.bfloat16)
    values_two = value_sum.astype(jnp.bfloat16)
    earlier_second = [
        from_behind((keys_two, values_two), "sp", distance) for distance in range(depth, 0, -1)
    ]
    key_ext_two = extend_rows(earlier_second, 0, keys_two)
    value_ext_two = extend_rows(earlier_second, 1, values_two)
    second = attend_band(queries_two, key_ext_two, value_ext_two, band_bias(rel_second), key_live)
    hidden_two = combine(second, out_second, hidden_one, post_second)
    return full_rows(hidden_two)


def scaled(values):
    return values * lax.rsqrt(jnp.mean(values * values, axis=-1, keepdims=True) + EPS)


def build_kernel(n, tok, head, width, reach):
    share = tok // 2
    cols = width // n
    span = reach + tok
    levels = n // 2
    depth = n * head
    dhalf = depth // 2
    wrows = width // n
    hrows = wrows // 2
    pieces = 4
    wide = width // pieces

    def kernel(
        q_hbm, k_hbm, v_hbm, wq_hbm, wk_hbm, wv_hbm, resid_hbm, o1_hbm, o2_hbm,
        rel1, rel2, post1, pre2, post2,
        out_ref,
        heads, weights, outs, res, bias, own_mix, mixed, parts, inbox, joined, branch, rows2, last,
        loc_sem, hs, hr, ws, wr, wf, mzs, mzr, mys, myr, ozs, ozr, oxs, oxr,
        ps, pr, bs, br, rzs, rzr, rys, ryr, rds, rdr, fs, fr,
    ):
        s = lax.axis_index("sp")
        t = lax.axis_index("tp")
        g = lax.axis_index("grp")
        u = 1 - t
        z = s // 2
        y = lax.rem(s, 2)
        v = 1 - y
        side = 2 * z + v
        turn = 1 - 2 * lax.rem(z, 2)

        def rcopy(src, dst, ssem, rsem, sp, tp, grp=g):
            return pltpu.make_async_remote_copy(
                src_ref=src, dst_ref=dst, send_sem=ssem, recv_sem=rsem,
                device_id={"grp": grp, "sp": sp, "tp": tp}, device_id_type=MESH,
            )

        def peer(k):
            return lax.rem(s + k, n)

        def near_level(i):
            return lax.rem(z + turn * i + levels, levels)

        def arrived(ref, sem):
            pltpu.make_async_copy(ref, ref, sem).wait()

        barrier = pltpu.get_barrier_semaphore()
        for k in range(1, n):
            pl.semaphore_signal(
                barrier, inc=1, device_id={"grp": g, "sp": peer(k), "tp": t}, device_id_type=MESH
            )
        pl.semaphore_signal(
            barrier, inc=1, device_id={"grp": g, "sp": s, "tp": u}, device_id_type=MESH
        )
        pl.semaphore_signal(
            barrier, inc=1, device_id={"grp": 1 - g, "sp": s, "tp": t}, device_id_type=MESH
        )
        pl.semaphore_wait(barrier, n + 1)

        def lanes(j):
            return pl.ds(pl.multiple_of(j * head, head), head)

        def trows(j, base=0):
            return pl.ds(pl.multiple_of(base + j * tok, tok), tok)

        qkv = (q_hbm, k_hbm, v_hbm)
        wqkv = (wq_hbm, wk_hbm, wv_hbm)
        out_hbm = (o1_hbm, o2_hbm)

        def head_copy(i, j):
            dst = heads.at[i, trows(s, reach)]
            return rcopy(qkv[i].at[:, lanes(j)], dst, hs, hr.at[s], j, t)

        def weight_half(src, part):
            start = pl.multiple_of(src * wrows + part * hrows, hrows)
            return weights.at[pl.ds(start, hrows)]

        def weight_copy(i, j):
            start = pl.multiple_of(s * wrows + g * hrows, hrows)
            piece = wqkv[i].at[pl.ds(pl.multiple_of(g * hrows, hrows), hrows), lanes(j)]
            dst = weights.at[pl.ds(start, hrows), pl.ds(i * head, head)]
            return rcopy(piece, dst, ws, wr.at[s, g], j, t)

        def weight_hand(src):
            piece = weight_half(src, g)
            return rcopy(piece, piece, wf, wr.at[src, g], s, t, 1 - g)

        def out_half(layer, c, part):
            return outs.at[layer, c, pl.ds(pl.multiple_of(part * dhalf, dhalf), dhalf)]

        def out_own(layer, to):
            piece = out_hbm[layer].at[pl.ds(pl.multiple_of(g * dhalf, dhalf), dhalf)]
            return rcopy(
                piece, out_half(layer, z, g), ozs.at[layer], ozr.at[layer, z], 2 * to + y, t
            )

        def out_pass(layer, c, to):
            piece = out_half(layer, c, g)
            return rcopy(piece, piece, ozs.at[layer], ozr.at[layer, c], 2 * to + y, t)

        def out_hand(layer, c):
            piece = out_half(layer, c, g)
            return rcopy(piece, piece, oxs.at[layer], oxr.at[layer, c], s, t, 1 - g)

        def out_start(layer):
            @pl.when(z < levels - 1)
            def _():
                out_own(layer, z + 1).start()

            @pl.when(z > 0)
            def _():
                out_own(layer, z - 1).start()

        def out_hop(layer, d):
            @pl.when(z >= d)
            def _():
                arrived(out_half(layer, z - d, g), ozr.at[layer, z - d])

                @pl.when(z < levels - 1)
                def _():
                    out_pass(layer, z - d, z + 1).start()

                out_hand(layer, z - d).start()

            @pl.when(z + d < levels)
            def _():
                arrived(out_half(layer, z + d, g), ozr.at[layer, z + d])

                @pl.when(z > 0)
                def _():
                    out_pass(layer, z + d, z - 1).start()

                out_hand(layer, z + d).start()

        def out_drain(layer):
            for at in range(levels):
                count = (1 + at if at < levels - 1 else 0) + (levels - at if at > 0 else 0)
                block = rows2.at[pl.ds(0, count)]

                @pl.when(z == at)
                def _():
                    arrived(block, ozs.at[layer])

            arrived(rows2.at[pl.ds(0, levels - 1)], oxs.at[layer])

        out_start(0)
        for k in range(1, n):
            for i in range(3):
                head_copy(i, peer(k)).start()
        for i in range(3):
            pltpu.make_async_copy(
                qkv[i].at[:, lanes(s)], heads.at[i, trows(s, reach)], hr.at[s]
            ).start()
        for i in range(3):
            pltpu.make_async_copy(
                wqkv[i].at[:, lanes(s)],
                weights.at[pl.ds(pl.multiple_of(s * wrows, wrows), wrows), pl.ds(i * head, head)],
                wr.at[s, 0],
            ).start()
        local = [
            pltpu.make_async_copy(o1_hbm, outs.at[0, z], loc_sem.at[0]),
            pltpu.make_async_copy(o2_hbm, outs.at[1, z], loc_sem.at[1]),
            pltpu.make_async_copy(
                resid_hbm.at[pl.ds(pl.multiple_of(t * share, share), share)], res, loc_sem.at[2]
            ),
        ]
        for copy in local:
            copy.start()

        near = 2 * REL_CLIP
        query = lax.broadcasted_iota(jnp.int32, (tok, span), 0) // SEG
        key = lax.broadcasted_iota(jnp.int32, (tok, span), 1) // SEG
        live = (key >= query) & (key <= query + LEFT)
        for layer, rel in enumerate((rel1, rel2)):
            table = rel[pl.ds(s, 1), :]
            top = table[:, near : near + 1]
            entry = lax.broadcasted_iota(jnp.int32, (near, near + tok), 0)
            place = lax.broadcasted_iota(jnp.int32, (near, near + tok), 1)
            flip = (entry + place == near).astype(F32)
            line = jnp.dot(
                jnp.broadcast_to(table[:, :near], (8, near)), flip,
                preferred_element_type=F32, precision=lax.Precision.HIGHEST,
            )[:1]
            spot = lax.broadcasted_iota(jnp.int32, line.shape, 1)
            line = jnp.where((spot == 0) | (spot >= near), top, line)
            spread = jnp.broadcast_to(line, (tok, near + tok))
            row = lax.broadcasted_iota(jnp.int32, spread.shape, 0)
            step = 1
            while step < tok:
                moved = pltpu.roll(spread, step, 1)
                spread = jnp.where(lax.rem(row // step, 2) == 1, moved, spread)
                step *= 2
            far = jnp.broadcast_to(top, (tok, span - near))
            whole = jnp.concatenate([far, spread[:, :near]], axis=1)
            bias[layer] = jnp.where(live, whole, NEG_FILL)

        heads[1, :reach] = jnp.zeros((reach, head), BF16)
        heads[2, :reach] = jnp.zeros((reach, head), BF16)

        def attend(layer, b):
            qb = heads[0, trows(b, reach)]
            kb = heads[1, pl.ds(pl.multiple_of(b * tok, tok), span)]
            vb = heads[2, pl.ds(pl.multiple_of(b * tok, tok), span)]
            scores = lax.dot_general(
                qb, kb, (((1,), (1,)), ((), ())), preferred_element_type=F32
            ) * head ** (-0.5) + bias[layer]
            column = lax.broadcasted_iota(jnp.int32, scores.shape, 1)
            scores = jnp.where(column >= reach - b * tok, scores, NEG_FILL)
            e = jnp.exp(scores - jnp.max(scores, axis=-1, keepdims=True))
            e = (e * (1.0 / jnp.sum(e, axis=-1, keepdims=True))).astype(BF16)
            return jnp.dot(e, vb, preferred_element_type=F32).astype(BF16)

        def mix_z(layer, b):
            dst = mixed.at[layer, s, trows(lax.rem(b, 2))]
            return rcopy(
                own_mix.at[layer, b], dst, mzs.at[layer], mzr.at[layer, z], 2 * (b // 2) + y, t
            )

        def mix_y(layer, c):
            block = mixed.at[layer, 2 * c + y]
            return rcopy(block, block, mys.at[layer], myr.at[layer, c], side, t)

        def one_head(layer, order, wait_block):
            def one(i, _):
                b = order(i)
                wait_block(b)
                result = attend(layer, b)

                @pl.when(b // 2 != z)
                def _():
                    own_mix[layer, b] = result
                    mix_z(layer, b).start()

                @pl.when(b // 2 == z)
                def _():
                    mixed[layer, s, trows(lax.rem(b, 2))] = result

                    @pl.when(lax.rem(b, 2) == 1)
                    def _():
                        mix_y(layer, z).start()

                return 0

            return one

        def forward_mix(layer):
            def one(i, _):
                c = near_level(i)
                arrived(mixed.at[layer, 2 * c + y], mzr.at[layer, c])
                mix_y(layer, c).start()
                return 0

            lax.fori_loop(1, levels, one, 0)

        def pcopy(layer, c):
            return rcopy(
                parts.at[layer, c, u], inbox.at[layer, c],
                ps.at[layer], pr.at[layer, c], s, u,
            )

        def bcopy(layer, c):
            return rcopy(
                joined.at[layer, c, v], branch.at[layer, y, c], bs.at[layer], br.at[layer], side, t
            )

        def project_branch(layer):
            for c in range(levels):
                arrived(mixed.at[layer, 2 * c + v], myr.at[layer, c])
            local[layer].wait()

            def project(c):
                @pl.when(c != z)
                def _():
                    arrived(out_half(layer, c, 1 - g), oxr.at[layer, c])

                lhs = jnp.concatenate([mixed[layer, j] for j in range(n)], axis=1)
                part = jnp.dot(lhs, outs[layer, c], preferred_element_type=F32).astype(BF16)
                for p in range(2):
                    for q in range(2):
                        parts[layer, c, q, p] = part[p * tok + q * share : p * tok + (q + 1) * share]
                pcopy(layer, c).start()

            def join(c):
                arrived(inbox.at[layer, c], pr.at[layer, c])
                both = parts[layer, c, t].astype(F32) + inbox[layer, c].astype(F32)
                joined[layer, c] = both.astype(BF16)
                bcopy(layer, c).start()
                branch[layer, y, c] = joined[layer, c, y]

            def step(i, _):
                project(near_level(i))

                @pl.when(i > 0)
                def _():
                    join(near_level(i - 1))

                return 0

            lax.fori_loop(0, levels, step, 0)
            join(near_level(levels - 1))
            arrived(branch.at[layer, v], br.at[layer])
            values = jnp.concatenate(
                [branch[layer, j % 2, j // 2] for j in range(n)], axis=1
            )
            return values.astype(F32)

        def branch_drain(layer):
            arrived(own_mix.at[layer, pl.ds(0, n - 2)], mzs.at[layer])
            arrived(mixed.at[layer, pl.ds(0, levels)], mys.at[layer])
            arrived(inbox.at[layer], ps.at[layer])
            arrived(branch.at[layer, 0], bs.at[layer])

        def heads_ready(b):
            arrived(heads.at[:, trows(b, reach)], hr.at[b])

        out_hop(0, 1)
        lax.fori_loop(0, n, one_head(0, lambda i: i, heads_ready), 0)
        out_hop(0, 2)
        forward_mix(0)
        for k in range(1, n):
            for i in range(3):
                weight_copy(i, peer(k)).start()
        for d in range(3, levels):
            out_hop(0, d)
        values = project_branch(0)
        local[2].wait()
        hidden = (res[...].astype(F32) + scaled(values) * post1[...]).astype(BF16)
        res[...] = hidden
        rows2[2 * s + t] = (scaled(hidden.astype(F32)) * pre2[...]).astype(BF16)

        def piece_of(item, m):
            return rows2.at[item, :, pl.ds(pl.multiple_of(m * wide, wide), wide)]

        def row_z(c, m, to):
            block = piece_of(2 * (2 * c + y) + t, m)
            return rcopy(block, block, rzs, rzr.at[c, m], 2 * to + y, t)

        def row_y(c, m):
            block = piece_of(2 * (2 * c + y) + t, m)
            return rcopy(block, block, rys, ryr.at[c, m], side, t)

        def row_d(src, m):
            block = piece_of(2 * src + t, m)
            return rcopy(block, block, rds, rdr.at[src], s, u)

        def own_rows(m, _):
            @pl.when(z < levels - 1)
            def _():
                row_z(z, m, z + 1).start()

            @pl.when(z > 0)
            def _():
                row_z(z, m, z - 1).start()

            row_y(z, m).start()
            row_d(s, m).start()
            return 0

        lax.fori_loop(0, pieces, own_rows, 0)
        out_start(1)

        def hand_weights(k, _):
            src = peer(k)
            arrived(weight_half(src, g), wr.at[src, g])
            weight_hand(src).start()
            return 0

        lax.fori_loop(1, n, hand_weights, 0)

        def from_level(c, m, on, to):
            arrived(piece_of(2 * (2 * c + y) + t, m), rzr.at[c, m])

            @pl.when(on)
            def _():
                row_z(c, m, to).start()

            row_y(c, m).start()
            row_d(2 * c + y, m).start()

        def from_side(c, m):
            arrived(piece_of(2 * (2 * c + v) + t, m), ryr.at[c, m])
            row_d(2 * c + v, m).start()

        def rows_hop(d):
            def one(m, _):
                if d < levels:
                    @pl.when(z >= d)
                    def _():
                        from_level(z - d, m, z < levels - 1, z + 1)

                    @pl.when(z + d < levels)
                    def _():
                        from_level(z + d, m, z > 0, z - 1)

                if d == 1:
                    from_side(z, m)
                else:
                    @pl.when(z >= d - 1)
                    def _():
                        from_side(z - (d - 1), m)

                    @pl.when(z + d - 1 < levels)
                    def _():
                        from_side(z + (d - 1), m)

                return 0

            lax.fori_loop(0, pieces, one, 0)

        def by_distance(i):
            low = jnp.minimum(z, levels - 1 - z)
            c = jnp.where(i <= low, low - i, i)
            return jnp.where(2 * z < levels, c, levels - 1 - c)

        def weights_ready(k, _):
            src = peer(k)
            arrived(weight_half(src, 1 - g), wr.at[src, 1 - g])
            return 0


        def project_rows(i, _):
            c = by_distance(i)
            arrived(rows2.at[4 * c + u], rdr.at[2 * c])
            arrived(rows2.at[4 * c + 2 + u], rdr.at[2 * c + 1])
            lhs = rows2[pl.ds(4 * c, 4)].reshape(2 * tok, width)
            both = jnp.dot(lhs, weights[...], preferred_element_type=F32).astype(BF16)
            start = pl.ds(pl.multiple_of(reach + c * 2 * tok, tok), 2 * tok)
            for i in range(3):
                heads[i, start] = both[:, i * head : (i + 1) * head]
            return 0

        def weights_here():
            lax.fori_loop(1, n, weights_ready, 0)
            arrived(weights.at[pl.ds(pl.multiple_of(s * wrows, wrows), wrows)], wr.at[s, 0])

        lag = reach // tok
        top = z == levels - 1
        start = jnp.where(top, lag + 2, jnp.where(z == 0, 0, 2 * z + 2))
        early = jnp.where(top, n - 2 - lag, jnp.where(z == 0, n - 2, n))
        known = jnp.where(top | (z == 0), levels - 1, levels)
        head_two = one_head(1, lambda i: lax.rem(start + i, n), lambda b: None)

        for d in range(1, levels + 1):
            rows_hop(d)
            if d == 2:
                out_hop(1, 1)
                weights_here()
                lax.fori_loop(0, 2, project_rows, 0)
            if d == levels - 1:
                out_hop(1, 2)
                lax.fori_loop(2, known, project_rows, 0)
                lax.fori_loop(0, early, head_two, 0)
        lax.fori_loop(known, levels, project_rows, 0)
        lax.fori_loop(early, n, head_two, 0)
        forward_mix(1)
        if levels > 2:
            out_hop(1, levels - 1)
        values = project_branch(1)
        done = (res[...].astype(F32) + scaled(values) * post2[...]).astype(BF16)
        last[t] = done
        final = rcopy(last.at[t], last.at[t], fs, fr, s, u)
        final.start()

        arrived(heads.at[:, pl.ds(reach, (n - 1) * tok)], hs)
        arrived(weights.at[pl.ds(0, (n - 1) * hrows)], ws)
        arrived(weights.at[pl.ds(0, (n - 1) * hrows)], wf)
        for layer in range(2):
            out_drain(layer)
            branch_drain(layer)
        for at in range(levels):
            count = (1 + at if at < levels - 1 else 0) + (levels - at if at > 0 else 0)
            block = rows2.at[pl.ds(0, count)]

            @pl.when(z == at)
            def _():
                arrived(block, rzs)

        arrived(rows2.at[pl.ds(0, levels)], rys)
        arrived(rows2.at[pl.ds(0, n)], rds)
        final.wait_send()
        rcopy(last.at[u], last.at[u], fs, fr, s, u).wait_recv()
        out_ref[:share] = last[0]
        out_ref[share:] = last[1]

    dma = pltpu.SemaphoreType.DMA
    scratch = [
        pltpu.VMEM((3, reach + n * tok, head), BF16),
        pltpu.VMEM((width, 3 * head), BF16),
        pltpu.VMEM((2, levels, depth, cols), BF16),
        pltpu.VMEM((share, width), BF16),
        pltpu.VMEM((2, tok, span), F32),
        pltpu.VMEM((2, n, tok, head), BF16),
        pltpu.VMEM((2, n, 2 * tok, head), BF16),
        pltpu.VMEM((2, levels, 2, 2, share, cols), BF16),
        pltpu.VMEM((2, levels, 2, share, cols), BF16),
        pltpu.VMEM((2, levels, 2, share, cols), BF16),
        pltpu.VMEM((2, 2, levels, share, cols), BF16),
        pltpu.VMEM((2 * n, share, width), BF16),
        pltpu.VMEM((2, share, width), BF16),
        dma((3,)),
        dma, dma((n,)),
        dma, dma((n, 2)), dma,
        dma((2,)), dma((2, levels)), dma((2,)), dma((2, levels)),
        dma((2,)), dma((2, levels)), dma((2,)), dma((2, levels)),
        dma((2,)), dma((2, levels)), dma((2,)), dma((2,)),
        dma, dma((levels, pieces)), dma, dma((levels, pieces)), dma, dma((n,)),
        dma, dma,
    ]
    return kernel, scratch


def by_heads(
    resid, queries_first, keys_first, values_first, rel_first, post_first, out_first, pre_second,
    query_weight, key_weight, value_weight, rel_second, post_second, out_second,
):
    n = lax.axis_size("sp")
    tok, width = resid.shape
    head = queries_first.shape[1] // rel_first.shape[0]
    kernel, scratch = build_kernel(n, tok, head, width, REACH)
    hbm = pl.BlockSpec(memory_space=pltpu.HBM)
    vmem = pl.BlockSpec(memory_space=pltpu.VMEM)
    return pl.pallas_call(
        kernel,
        out_shape=jax.ShapeDtypeStruct((tok, width), BF16),
        in_specs=[hbm] * 9 + [vmem] * 5,
        out_specs=vmem,
        scratch_shapes=scratch,
        compiler_params=pltpu.CompilerParams(
            collective_id=0, has_side_effects=True, vmem_limit_bytes=60 * 2**20
        ),
    )(
        queries_first, keys_first, values_first, query_weight, key_weight, value_weight, resid,
        out_first, out_second, rel_first, rel_second,
        post_first[None], pre_second[None], post_second[None],
    )


def solution(mesh):
    in_specs = (
        P(("grp", "sp"), None),
        P(("grp", "sp"), "tp"),
        P(("grp", "sp"), "tp"),
        P(("grp", "sp"), "tp"),
        P("tp", None),
        P(),
        P("tp", "sp"),
        P(),
        P("sp", "tp"),
        P("sp", "tp"),
        P("sp", "tp"),
        P("tp", None),
        P(),
        P("tp", "sp"),
    )
    out_specs = P(("grp", "sp"), None)
    return jax.shard_map(shards, mesh=mesh, in_specs=in_specs, out_specs=out_specs, check_vma=False)
```

```python
import jax
import jax.numpy as jnp
from jax import lax
from jax.experimental import pallas as pl
from jax.experimental.pallas import tpu as pltpu
from jax.sharding import PartitionSpec as P

MESH = pl.DeviceIdType.MESH
BF16 = jnp.bfloat16
F32 = jnp.float32

SEG = 64
LEFT = 8
REACH = 512
REL_CLIP = 128


EPS = 1e-06
NEG_FILL = -1e30


def from_behind(value, axis, steps):
    count = lax.axis_size(axis)
    initial, last = (max(0, -steps), min(count, count - steps))
    return lax.ppermute(value, axis, [(source, source + steps) for source in range(initial, last)])


def band_bias(bias_table):
    heads_here = bias_table.shape[0]
    band = (LEFT + 1) * SEG
    length = SEG + band
    index = jnp.arange(length, dtype=jnp.int32)
    distance = jnp.where(index < band, LEFT * SEG - index, LEFT * SEG + length - index)
    slot = jnp.clip(distance, -REL_CLIP, REL_CLIP) + REL_CLIP
    onehot = (slot[:, None] == jnp.arange(2 * REL_CLIP + 1, dtype=jnp.int32)[None, :]).astype(
        jnp.float32
    )
    diagonal_values = jnp.dot(bias_table, onehot.T, precision=lax.Precision.HIGHEST)
    spread = jnp.broadcast_to(diagonal_values[:, None, :], (heads_here, SEG, length)).reshape(
        heads_here, SEG * length
    )
    return spread[:, : SEG * (length - 1)].reshape(heads_here, SEG, length - 1)[:, :, :band]


def attend_band(queries, key_rows, value_rows, bias, key_live):
    rows, width = queries.shape
    heads_here = bias.shape[0]
    head_size = width // heads_here
    blocks = rows // SEG
    query_seg = queries.reshape(blocks, SEG, heads_here, head_size)
    key_seg = key_rows.reshape(blocks + LEFT, SEG, heads_here, head_size)
    value_seg = value_rows.reshape(blocks + LEFT, SEG, heads_here, head_size)
    live_seg = key_live.reshape(blocks + LEFT, SEG)
    key_band = jnp.concatenate(
        [key_seg[earlier : earlier + blocks] for earlier in range(LEFT + 1)], axis=1
    )
    value_band = jnp.concatenate(
        [value_seg[earlier : earlier + blocks] for earlier in range(LEFT + 1)], axis=1
    )
    live_band = jnp.concatenate(
        [live_seg[earlier : earlier + blocks] for earlier in range(LEFT + 1)], axis=1
    )
    scores = jnp.einsum("nqhd,nkhd->nhqk", query_seg, key_band, preferred_element_type=jnp.float32)
    scores = scores * head_size ** (-0.5) + bias[None]
    scores = jnp.where(live_band[:, None, None, :], scores, NEG_FILL)
    largest = jnp.max(scores, axis=-1, keepdims=True)
    weights = jnp.exp(scores - largest)
    weights = (weights / jnp.sum(weights, axis=-1, keepdims=True)).astype(jnp.bfloat16)
    mixed = jnp.einsum("nhqk,nkhd->nqhd", weights, value_band, preferred_element_type=jnp.float32)
    return mixed.astype(jnp.bfloat16).reshape(rows, width)


def extend_rows(pieces, member, own_rows):
    joined = jnp.concatenate([piece[member] for piece in pieces] + [own_rows], axis=0)
    return joined


def normed(hidden, gain):
    values = hidden.astype(jnp.float32)
    scale = lax.rsqrt(jnp.mean(values * values, axis=-1, keepdims=True) + EPS)
    return (values * scale * gain).astype(jnp.bfloat16)


def residual_add(branch, residual, gain):
    values = branch.astype(jnp.float32)
    scale = lax.rsqrt(jnp.mean(values * values, axis=-1, keepdims=True) + EPS)
    return (residual.astype(jnp.float32) + values * scale * gain).astype(jnp.bfloat16)


def combine(mixed, weight, residual, gain):
    partial_rows = jnp.dot(
        mixed, lax.all_gather(weight, "sp", axis=1, tiled=True), preferred_element_type=jnp.float32
    )
    branch = lax.psum_scatter(
        partial_rows.astype(jnp.bfloat16), "tp", scatter_dimension=0, tiled=True
    )
    return residual_add(branch, residual, gain)


def full_rows(share):
    return lax.all_gather(share, "tp", axis=0, tiled=True)


def shards(
    resid,
    queries_first,
    keys_first,
    values_first,
    rel_first,
    post_first,
    out_first,
    pre_second,
    query_weight,
    key_weight,
    value_weight,
    rel_second,
    post_second,
    out_second,
):
    tok_rows = resid.shape[0]
    n_sp = lax.axis_size("sp")
    if (
        rel_first.shape[0] == n_sp
        and n_sp % 2 == 0
        and lax.axis_size("tp") == 2
        and lax.axis_size("grp") == 2
        and REACH % tok_rows == 0
        and tok_rows == REL_CLIP
    ):
        return by_heads(
            resid, queries_first, keys_first, values_first, rel_first, post_first, out_first,
            pre_second, query_weight, key_weight, value_weight, rel_second, post_second, out_second,
        )
    depth = (REACH + tok_rows - 1) // tok_rows
    anchor = lax.axis_index("sp") * tok_rows
    key_live = anchor - REACH + jnp.arange(tok_rows + REACH, dtype=jnp.int32) >= 0
    share_rows = tok_rows // lax.axis_size("tp")
    base_rows = lax.dynamic_slice_in_dim(resid, lax.axis_index("tp") * share_rows, share_rows, 0)
    earlier_first = [
        from_behind((keys_first, values_first), "sp", distance) for distance in range(depth, 0, -1)
    ]
    key_ext = extend_rows(earlier_first, 0, keys_first)
    value_ext = extend_rows(earlier_first, 1, values_first)
    first = attend_band(queries_first, key_ext, value_ext, band_bias(rel_first), key_live)
    hidden_one = combine(first, out_first, base_rows, post_first)
    inputs_two = full_rows(normed(hidden_one, pre_second))
    query_sum = jnp.dot(
        inputs_two,
        lax.all_gather(query_weight, "sp", axis=0, tiled=True),
        preferred_element_type=jnp.float32,
    )
    key_sum = jnp.dot(
        inputs_two,
        lax.all_gather(key_weight, "sp", axis=0, tiled=True),
        preferred_element_type=jnp.float32,
    )
    value_sum = jnp.dot(
        inputs_two,
        lax.all_gather(value_weight, "sp", axis=0, tiled=True),
        preferred_element_type=jnp.float32,
    )
    queries_two = query_sum.astype(jnp.bfloat16)
    keys_two = key_sum.astype(jnp.bfloat16)
    values_two = value_sum.astype(jnp.bfloat16)
    earlier_second = [
        from_behind((keys_two, values_two), "sp", distance) for distance in range(depth, 0, -1)
    ]
    key_ext_two = extend_rows(earlier_second, 0, keys_two)
    value_ext_two = extend_rows(earlier_second, 1, values_two)
    second = attend_band(queries_two, key_ext_two, value_ext_two, band_bias(rel_second), key_live)
    hidden_two = combine(second, out_second, hidden_one, post_second)
    return full_rows(hidden_two)


def scaled(values):
    return values * lax.rsqrt(jnp.mean(values * values, axis=-1, keepdims=True) + EPS)


def build_kernel(n, tok, head, width, reach):
    share = tok // 2
    cols = width // n
    span = reach + tok
    levels = n // 2
    depth = n * head
    dhalf = depth // 2
    wrows = width // n
    hrows = wrows // 2
    pieces = 4
    cuts = 2
    wide = width // pieces

    def kernel(
        q_hbm, k_hbm, v_hbm, wq_hbm, wk_hbm, wv_hbm, resid_hbm, o1_hbm, o2_hbm,
        rel1, rel2, post1, pre2, post2,
        out_ref,
        heads, weights, outs, res, bias, own_mix, mixed, parts, inbox, joined, branch, rows2, last,
        loc_sem, hs, hr, ws, wr, wf, mzs, mzr, mys, myr, ozs, ozr, oxs, oxr,
        ms, mr, ns, nr, nxs, nxr, ps, pr, bs, br, rzs, rzr, rys, ryr, rds, rdr, fs, fr,
    ):
        s = lax.axis_index("sp")
        t = lax.axis_index("tp")
        g = lax.axis_index("grp")
        u = 1 - t
        z = s // 2
        y = lax.rem(s, 2)
        v = 1 - y
        side = 2 * z + v
        turn = 1 - 2 * lax.rem(z, 2)
        rung = lax.rem(z, 2)
        twin = z + 1 - 2 * rung
        across = lax.rem(z + levels // 2, levels)

        def rcopy(src, dst, ssem, rsem, sp, tp, grp=g):
            return pltpu.make_async_remote_copy(
                src_ref=src, dst_ref=dst, send_sem=ssem, recv_sem=rsem,
                device_id={"grp": grp, "sp": sp, "tp": tp}, device_id_type=MESH,
            )

        def peer(k):
            return lax.rem(s + k, n)

        def near_level(i):
            return lax.rem(z + turn * i + levels, levels)

        def by_distance(i):
            low = jnp.minimum(z, levels - 1 - z)
            c = jnp.where(i <= low, low - i, i)
            return jnp.where(2 * z < levels, c, levels - 1 - c)

        def arrived(ref, sem):
            pltpu.make_async_copy(ref, ref, sem).wait()

        barrier = pltpu.get_barrier_semaphore()
        for k in range(1, n):
            pl.semaphore_signal(
                barrier, inc=1, device_id={"grp": g, "sp": peer(k), "tp": t}, device_id_type=MESH
            )
        pl.semaphore_signal(
            barrier, inc=1, device_id={"grp": g, "sp": s, "tp": u}, device_id_type=MESH
        )
        pl.semaphore_signal(
            barrier, inc=1, device_id={"grp": 1 - g, "sp": s, "tp": t}, device_id_type=MESH
        )
        pl.semaphore_wait(barrier, n + 1)

        def lanes(j):
            return pl.ds(pl.multiple_of(j * head, head), head)

        def trows(j, base=0):
            return pl.ds(pl.multiple_of(base + j * tok, tok), tok)

        qkv = (q_hbm, k_hbm, v_hbm)
        wqkv = (wq_hbm, wk_hbm, wv_hbm)

        def head_copy(i, j):
            dst = heads.at[i, trows(s, reach)]
            return rcopy(qkv[i].at[:, lanes(j)], dst, hs, hr.at[s], j, t)

        def weight_half(src, part):
            start = pl.multiple_of(src * wrows + part * hrows, hrows)
            return weights.at[pl.ds(start, hrows)]

        def weight_copy(i, j):
            start = pl.multiple_of(s * wrows + g * hrows, hrows)
            piece = wqkv[i].at[pl.ds(pl.multiple_of(g * hrows, hrows), hrows), lanes(j)]
            dst = weights.at[pl.ds(start, hrows), pl.ds(i * head, head)]
            return rcopy(piece, dst, ws, wr.at[s, g], j, t)

        def weight_hand(src):
            piece = weight_half(src, g)
            return rcopy(piece, piece, wf, wr.at[src, g], s, t, 1 - g)

        dcut = dhalf // cuts

        def out_half(c, part):
            return outs.at[0, c, pl.ds(pl.multiple_of(part * dhalf, dhalf), dhalf)]

        def out_piece(c, h):
            return outs.at[0, c, pl.ds(pl.multiple_of(g * dhalf + h * dcut, dcut), dcut)]

        def out_own(h, to):
            piece = o1_hbm.at[pl.ds(pl.multiple_of(g * dhalf + h * dcut, dcut), dcut)]
            return rcopy(piece, out_piece(z, h), ozs, ozr.at[z, h], 2 * to + y, t)

        def out_pass(c, h, to):
            piece = out_piece(c, h)
            return rcopy(piece, piece, ozs, ozr.at[c, h], 2 * to + y, t)

        def out_hand(c, h):
            piece = out_piece(c, h)
            return rcopy(piece, piece, oxs, oxr.at[c], s, t, 1 - g)

        def out_start():
            for h in range(cuts):
                @pl.when(z < levels - 1)
                def _():
                    out_own(h, z + 1).start()

                @pl.when(z > 0)
                def _():
                    out_own(h, z - 1).start()

        def out_hop(d):
            for h in range(cuts):
                @pl.when(z >= d)
                def _():
                    arrived(out_piece(z - d, h), ozr.at[z - d, h])

                    @pl.when(z < levels - 1)
                    def _():
                        out_pass(z - d, h, z + 1).start()

                    out_hand(z - d, h).start()

                @pl.when(z + d < levels)
                def _():
                    arrived(out_piece(z + d, h), ozr.at[z + d, h])

                    @pl.when(z > 0)
                    def _():
                        out_pass(z + d, h, z - 1).start()

                    out_hand(z + d, h).start()

        def two_half(e, part):
            return outs.at[1, e, pl.ds(pl.multiple_of(part * dhalf, dhalf), dhalf)]

        def two_own(e, sp):
            piece = o2_hbm.at[pl.ds(pl.multiple_of(g * dhalf, dhalf), dhalf)]
            return rcopy(piece, two_half(e, g), ns, nr.at[e], sp, t)

        def two_side():
            piece = two_half(2 + y, g)
            return rcopy(piece, piece, ns, nr.at[2 + y], side, t)

        def two_hand(e):
            piece = two_half(e, g)
            return rcopy(piece, piece, nxs, nxr.at[e], s, t, 1 - g)

        def two_start():
            two_own(2 + y, 2 * across + y).start()

        def two_near():
            arrived(two_half(2 + y, g), nr.at[2 + y])
            two_side().start()
            two_hand(2 + y).start()

        def two_far():
            arrived(two_half(2 + v, g), nr.at[2 + v])
            two_hand(2 + v).start()

        def out_drain():
            for at in range(levels):
                count = (1 + at if at < levels - 1 else 0) + (levels - at if at > 0 else 0)
                block = rows2.at[pl.ds(0, count)]

                @pl.when(z == at)
                def _():
                    arrived(block, ozs)

            arrived(rows2.at[pl.ds(0, levels - 1)], oxs)

        out_start()
        for k in range(1, n):
            for i in range(3):
                head_copy(i, peer(k)).start()
        for i in range(3):
            pltpu.make_async_copy(
                qkv[i].at[:, lanes(s)], heads.at[i, trows(s, reach)], hr.at[s]
            ).start()
        for i in range(3):
            pltpu.make_async_copy(
                wqkv[i].at[:, lanes(s)],
                weights.at[pl.ds(pl.multiple_of(s * wrows, wrows), wrows), pl.ds(i * head, head)],
                wr.at[s, 0],
            ).start()
        two_own(y, side).start()
        local = [
            pltpu.make_async_copy(o1_hbm, outs.at[0, z], loc_sem.at[0]),
            pltpu.make_async_copy(o2_hbm, outs.at[1, y], loc_sem.at[1]),
            pltpu.make_async_copy(
                resid_hbm.at[pl.ds(pl.multiple_of(t * share, share), share)], res, loc_sem.at[2]
            ),
        ]
        for copy in local:
            copy.start()

        near = 2 * REL_CLIP
        query = lax.broadcasted_iota(jnp.int32, (tok, span), 0) // SEG
        key = lax.broadcasted_iota(jnp.int32, (tok, span), 1) // SEG
        live = (key >= query) & (key <= query + LEFT)
        for layer, rel in enumerate((rel1, rel2)):
            table = rel[pl.ds(s, 1), :]
            top = table[:, near : near + 1]
            entry = lax.broadcasted_iota(jnp.int32, (near, near + tok), 0)
            place = lax.broadcasted_iota(jnp.int32, (near, near + tok), 1)
            flip = (entry + place == near).astype(F32)
            line = jnp.dot(
                jnp.broadcast_to(table[:, :near], (8, near)), flip,
                preferred_element_type=F32, precision=lax.Precision.HIGHEST,
            )[:1]
            spot = lax.broadcasted_iota(jnp.int32, line.shape, 1)
            line = jnp.where((spot == 0) | (spot >= near), top, line)
            spread = jnp.broadcast_to(line, (tok, near + tok))
            row = lax.broadcasted_iota(jnp.int32, spread.shape, 0)
            step = 1
            while step < tok:
                moved = pltpu.roll(spread, step, 1)
                spread = jnp.where(lax.rem(row // step, 2) == 1, moved, spread)
                step *= 2
            far = jnp.broadcast_to(top, (tok, span - near))
            whole = jnp.concatenate([far, spread[:, :near]], axis=1)
            bias[layer] = jnp.where(live, whole, NEG_FILL)

        heads[1, :reach] = jnp.zeros((reach, head), BF16)
        heads[2, :reach] = jnp.zeros((reach, head), BF16)

        def attend(layer, b):
            qb = heads[0, trows(b, reach)]
            kb = heads[1, pl.ds(pl.multiple_of(b * tok, tok), span)]
            vb = heads[2, pl.ds(pl.multiple_of(b * tok, tok), span)]
            scores = lax.dot_general(
                qb, kb, (((1,), (1,)), ((), ())), preferred_element_type=F32
            ) * head ** (-0.5) + bias[layer]
            column = lax.broadcasted_iota(jnp.int32, scores.shape, 1)
            scores = jnp.where(column >= reach - b * tok, scores, NEG_FILL)
            e = jnp.exp(scores - jnp.max(scores, axis=-1, keepdims=True))
            e = (e * (1.0 / jnp.sum(e, axis=-1, keepdims=True))).astype(BF16)
            return jnp.dot(e, vb, preferred_element_type=F32).astype(BF16)

        def mix_z(layer, b):
            dst = mixed.at[layer, s, trows(lax.rem(b, 2))]
            return rcopy(
                own_mix.at[layer, b], dst, mzs.at[layer], mzr.at[layer, z], 2 * (b // 2) + y, t
            )

        def mix_y(layer, c):
            block = mixed.at[layer, 2 * c + y]
            return rcopy(block, block, mys.at[layer], myr.at[layer, c], side, t)

        def one_head(layer, order, wait_block):
            def one(i, _):
                b = order(i)
                wait_block(b)
                result = attend(layer, b)

                @pl.when(b // 2 != z)
                def _():
                    own_mix[layer, b] = result
                    mix_z(layer, b).start()

                @pl.when(b // 2 == z)
                def _():
                    mixed[layer, s, trows(lax.rem(b, 2))] = result

                    @pl.when(lax.rem(b, 2) == 1)
                    def _():
                        mix_y(layer, z).start()

                return 0

            return one

        def forward_mix(layer):
            def one(i, _):
                c = near_level(i)
                arrived(mixed.at[layer, 2 * c + y], mzr.at[layer, c])
                mix_y(layer, c).start()
                return 0

            lax.fori_loop(1, levels, one, 0)

        def two_copy(layer, b, level):
            dst = mixed.at[layer, s, trows(lax.rem(b // 2, 2))]
            return rcopy(
                own_mix.at[layer, b], dst, ms, mr,
                2 * level + lax.rem(b, 2), t,
            )

        def two_head(layer, order, wait_block):
            def one(i, _):
                b = order(i)
                wait_block(b)
                result = attend(layer, b)
                own_mix[layer, b] = result
                level = b // 2
                other = level + 1 - 2 * lax.rem(level, 2)
                mine = lax.rem(b, 2) == y

                @pl.when(jnp.logical_not(mine & (level == z)))
                def _():
                    two_copy(layer, b, level).start()

                @pl.when(jnp.logical_not(mine & (other == z)))
                def _():
                    two_copy(layer, b, other).start()

                @pl.when(mine & (level // 2 == z // 2))
                def _():
                    mixed[layer, s, trows(lax.rem(level, 2))] = result

                return 0

            return one

        def pcopy(layer, c):
            return rcopy(
                parts.at[layer, c, u], inbox.at[layer, c],
                ps.at[layer], pr.at[layer, c], s, u,
            )

        def bcopy(layer, c):
            if layer == 0:
                return rcopy(
                    joined.at[layer, c, v], branch.at[layer, y, c], bs.at[layer], br.at[layer],
                    side, t,
                )
            return rcopy(
                joined.at[layer, c, 1 - rung], branch.at[layer, rung, c],
                bs.at[layer], br.at[layer], 2 * twin + y, t,
            )

        def project_branch(layer):
            if layer == 0:
                for c in range(levels):
                    arrived(mixed.at[layer, 2 * c + v], myr.at[layer, c])
                own_block, mine, order = z, y, near_level
                hand_ready = lambda c: arrived(out_half(c, 1 - g), oxr.at[c])
            else:
                arrived(mixed.at[layer, pl.ds(0, n - 1)], mr)
                own_block, mine = y, rung
                order = lambda i: 2 * (i // 2) + lax.rem(y + i, 2)
                hand_ready = lambda e: arrived(two_half(e, 1 - g), nxr.at[e])
            local[layer].wait()

            def project(c):
                @pl.when(c != own_block)
                def _():
                    hand_ready(c)

                lhs = jnp.concatenate([mixed[layer, j] for j in range(n)], axis=1)
                part = jnp.dot(lhs, outs[layer, c], preferred_element_type=F32).astype(BF16)
                for p in range(2):
                    for q in range(2):
                        parts[layer, c, q, p] = part[p * tok + q * share : p * tok + (q + 1) * share]
                pcopy(layer, c).start()

            def join(c):
                arrived(inbox.at[layer, c], pr.at[layer, c])
                both = parts[layer, c, t].astype(F32) + inbox[layer, c].astype(F32)
                joined[layer, c] = both.astype(BF16)
                bcopy(layer, c).start()
                branch[layer, mine, c] = joined[layer, c, mine]

            def step(i, _):
                project(order(i))

                @pl.when(i > 0)
                def _():
                    join(order(i - 1))

                return 0

            lax.fori_loop(0, levels, step, 0)
            join(order(levels - 1))
            arrived(branch.at[layer, 1 - mine], br.at[layer])

            def column_block(j):
                if layer == 0:
                    return branch[layer, j % 2, j // 2]
                half = lax.rem(j // levels + 2 * z // levels, 2)
                return branch[layer, (j // 2) % 2, 2 * half + j % 2]

            values = jnp.concatenate([column_block(j) for j in range(n)], axis=1)
            return values.astype(F32)

        def branch_drain(layer):
            if layer == 0:
                arrived(own_mix.at[layer, pl.ds(0, n - 2)], mzs.at[layer])
                arrived(mixed.at[layer, pl.ds(0, levels)], mys.at[layer])
            else:
                arrived(mixed.at[layer, pl.ds(0, n - 1)], ms)
            arrived(inbox.at[layer], ps.at[layer])
            arrived(branch.at[layer, 0], bs.at[layer])

        def heads_ready(b):
            arrived(heads.at[:, trows(b, reach)], hr.at[b])

        out_hop(1)
        lax.fori_loop(0, n, one_head(0, lambda i: i, heads_ready), 0)
        out_hop(2)
        forward_mix(0)
        for k in range(1, n):
            for i in range(3):
                weight_copy(i, peer(k)).start()
        for d in range(3, levels):
            out_hop(d)
        values = project_branch(0)
        local[2].wait()
        hidden = (res[...].astype(F32) + scaled(values) * post1[...]).astype(BF16)
        res[...] = hidden
        rows2[2 * s + t] = (scaled(hidden.astype(F32)) * pre2[...]).astype(BF16)

        def piece_of(item, m):
            return rows2.at[item, :, pl.ds(pl.multiple_of(m * wide, wide), wide)]

        def row_z(c, m, to):
            block = piece_of(2 * (2 * c + y) + t, m)
            return rcopy(block, block, rzs, rzr.at[c, m], 2 * to + y, t)

        def row_y(c, m):
            block = piece_of(2 * (2 * c + y) + t, m)
            return rcopy(block, block, rys, ryr.at[c, m], side, t)

        def row_d(src, m):
            block = piece_of(2 * src + t, m)
            return rcopy(block, block, rds, rdr.at[src], s, u)

        def own_rows(m, _):
            @pl.when(z < levels - 1)
            def _():
                row_z(z, m, z + 1).start()

            @pl.when(z > 0)
            def _():
                row_z(z, m, z - 1).start()

            row_y(z, m).start()
            row_d(s, m).start()
            return 0

        lax.fori_loop(0, pieces, own_rows, 0)
        two_start()

        def hand_weights(k, _):
            src = peer(k)
            arrived(weight_half(src, g), wr.at[src, g])
            weight_hand(src).start()
            return 0

        lax.fori_loop(1, n, hand_weights, 0)
        arrived(two_half(v, g), nr.at[v])
        two_hand(v).start()

        def from_level(c, m, on, to):
            arrived(piece_of(2 * (2 * c + y) + t, m), rzr.at[c, m])

            @pl.when(on)
            def _():
                row_z(c, m, to).start()

            row_y(c, m).start()
            row_d(2 * c + y, m).start()

        def from_side(c, m):
            arrived(piece_of(2 * (2 * c + v) + t, m), ryr.at[c, m])
            row_d(2 * c + v, m).start()

        def rows_hop(d):
            def one(m, _):
                if d < levels:
                    @pl.when(z >= d)
                    def _():
                        from_level(z - d, m, z < levels - 1, z + 1)

                    @pl.when(z + d < levels)
                    def _():
                        from_level(z + d, m, z > 0, z - 1)

                if d == 1:
                    from_side(z, m)
                else:
                    @pl.when(z >= d - 1)
                    def _():
                        from_side(z - (d - 1), m)

                    @pl.when(z + d - 1 < levels)
                    def _():
                        from_side(z + (d - 1), m)

                return 0

            lax.fori_loop(0, pieces, one, 0)

        def weights_ready(k, _):
            src = peer(k)
            arrived(weight_half(src, 1 - g), wr.at[src, 1 - g])
            return 0


        def project_rows(i, _):
            c = by_distance(i)
            arrived(rows2.at[4 * c + u], rdr.at[2 * c])
            arrived(rows2.at[4 * c + 2 + u], rdr.at[2 * c + 1])
            lhs = rows2[pl.ds(4 * c, 4)].reshape(2 * tok, width)
            both = jnp.dot(lhs, weights[...], preferred_element_type=F32).astype(BF16)
            start = pl.ds(pl.multiple_of(reach + c * 2 * tok, tok), 2 * tok)
            for i in range(3):
                heads[i, start] = both[:, i * head : (i + 1) * head]
            return 0

        def weights_here():
            lax.fori_loop(1, n, weights_ready, 0)
            arrived(weights.at[pl.ds(pl.multiple_of(s * wrows, wrows), wrows)], wr.at[s, 0])

        lag = reach // tok
        top = z == levels - 1
        start = jnp.where(top, lag + 2, jnp.where(z == 0, 0, 2 * z + 2))
        early = jnp.where(top, n - 2 - lag, jnp.where(z == 0, n - 2, n))
        known = jnp.where(top | (z == 0), levels - 1, levels)
        head_two = two_head(1, lambda i: lax.rem(start + i, n), lambda b: None)

        for d in range(1, levels + 1):
            rows_hop(d)
            if d == 2:
                weights_here()
                lax.fori_loop(0, 2, project_rows, 0)
            if d == levels - 1:
                two_near()
                lax.fori_loop(2, known, project_rows, 0)
                lax.fori_loop(0, early, head_two, 0)
        lax.fori_loop(known, levels, project_rows, 0)
        lax.fori_loop(early, n, head_two, 0)
        two_far()
        values = project_branch(1)
        done = (res[...].astype(F32) + scaled(values) * post2[...]).astype(BF16)
        last[t] = done
        final = rcopy(last.at[t], last.at[t], fs, fr, s, u)
        final.start()

        arrived(heads.at[:, pl.ds(reach, (n - 1) * tok)], hs)
        arrived(weights.at[pl.ds(0, (n - 1) * hrows)], ws)
        arrived(weights.at[pl.ds(0, (n - 1) * hrows)], wf)
        out_drain()
        arrived(rows2.at[pl.ds(0, 3)], ns)
        arrived(rows2.at[pl.ds(0, 3)], nxs)
        for layer in range(2):
            branch_drain(layer)
        for at in range(levels):
            count = (1 + at if at < levels - 1 else 0) + (levels - at if at > 0 else 0)
            block = rows2.at[pl.ds(0, count)]

            @pl.when(z == at)
            def _():
                arrived(block, rzs)

        arrived(rows2.at[pl.ds(0, levels)], rys)
        arrived(rows2.at[pl.ds(0, n)], rds)
        final.wait_send()
        rcopy(last.at[u], last.at[u], fs, fr, s, u).wait_recv()
        out_ref[:share] = last[0]
        out_ref[share:] = last[1]

    dma = pltpu.SemaphoreType.DMA
    scratch = [
        pltpu.VMEM((3, reach + n * tok, head), BF16),
        pltpu.VMEM((width, 3 * head), BF16),
        pltpu.VMEM((2, levels, depth, cols), BF16),
        pltpu.VMEM((share, width), BF16),
        pltpu.VMEM((2, tok, span), F32),
        pltpu.VMEM((2, n, tok, head), BF16),
        pltpu.VMEM((2, n, 2 * tok, head), BF16),
        pltpu.VMEM((2, levels, 2, 2, share, cols), BF16),
        pltpu.VMEM((2, levels, 2, share, cols), BF16),
        pltpu.VMEM((2, levels, 2, share, cols), BF16),
        pltpu.VMEM((2, 2, levels, share, cols), BF16),
        pltpu.VMEM((2 * n, share, width), BF16),
        pltpu.VMEM((2, share, width), BF16),
        dma((3,)),
        dma, dma((n,)),
        dma, dma((n, 2)), dma,
        dma((1,)), dma((1, levels)), dma((1,)), dma((1, levels)),
        dma, dma((levels, cuts)), dma, dma((levels,)),
        dma, dma, dma, dma((levels,)), dma, dma((levels,)),
        dma((2,)), dma((2, levels)), dma((2,)), dma((2,)),
        dma, dma((levels, pieces)), dma, dma((levels, pieces)), dma, dma((n,)),
        dma, dma,
    ]
    return kernel, scratch


def by_heads(
    resid, queries_first, keys_first, values_first, rel_first, post_first, out_first, pre_second,
    query_weight, key_weight, value_weight, rel_second, post_second, out_second,
):
    n = lax.axis_size("sp")
    tok, width = resid.shape
    head = queries_first.shape[1] // rel_first.shape[0]
    kernel, scratch = build_kernel(n, tok, head, width, REACH)
    hbm = pl.BlockSpec(memory_space=pltpu.HBM)
    vmem = pl.BlockSpec(memory_space=pltpu.VMEM)
    return pl.pallas_call(
        kernel,
        out_shape=pltpu.VMEM((tok, width), BF16),
        in_specs=[hbm] * 9 + [vmem] * 5,
        out_specs=vmem,
        scratch_shapes=scratch,
        compiler_params=pltpu.CompilerParams(
            collective_id=0, has_side_effects=True, vmem_limit_bytes=60 * 2**20
        ),
    )(
        queries_first, keys_first, values_first, query_weight, key_weight, value_weight, resid,
        out_first, out_second, rel_first, rel_second,
        post_first[None], pre_second[None], post_second[None],
    )


def solution(mesh):
    in_specs = (
        P(("grp", "sp"), None),
        P(("grp", "sp"), "tp"),
        P(("grp", "sp"), "tp"),
        P(("grp", "sp"), "tp"),
        P("tp", None),
        P(),
        P("tp", "sp"),
        P(),
        P("sp", "tp"),
        P("sp", "tp"),
        P("sp", "tp"),
        P("tp", None),
        P(),
        P("tp", "sp"),
    )
    out_specs = P(("grp", "sp"), None)
    return jax.shard_map(shards, mesh=mesh, in_specs=in_specs, out_specs=out_specs, check_vma=False)
```

```python
import jax
import jax.numpy as jnp
from jax import lax
from jax.experimental import pallas as pl
from jax.experimental.pallas import tpu as pltpu
from jax.sharding import PartitionSpec as P

MESH = pl.DeviceIdType.MESH
BF16 = jnp.bfloat16
F32 = jnp.float32

SEG = 64
LEFT = 8
REACH = 512
REL_CLIP = 128


EPS = 1e-06
NEG_FILL = -1e30


def from_behind(value, axis, steps):
    count = lax.axis_size(axis)
    initial, last = (max(0, -steps), min(count, count - steps))
    return lax.ppermute(value, axis, [(source, source + steps) for source in range(initial, last)])


def band_bias(bias_table):
    heads_here = bias_table.shape[0]
    band = (LEFT + 1) * SEG
    length = SEG + band
    index = jnp.arange(length, dtype=jnp.int32)
    distance = jnp.where(index < band, LEFT * SEG - index, LEFT * SEG + length - index)
    slot = jnp.clip(distance, -REL_CLIP, REL_CLIP) + REL_CLIP
    onehot = (slot[:, None] == jnp.arange(2 * REL_CLIP + 1, dtype=jnp.int32)[None, :]).astype(
        jnp.float32
    )
    diagonal_values = jnp.dot(bias_table, onehot.T, precision=lax.Precision.HIGHEST)
    spread = jnp.broadcast_to(diagonal_values[:, None, :], (heads_here, SEG, length)).reshape(
        heads_here, SEG * length
    )
    return spread[:, : SEG * (length - 1)].reshape(heads_here, SEG, length - 1)[:, :, :band]


def attend_band(queries, key_rows, value_rows, bias, key_live):
    rows, width = queries.shape
    heads_here = bias.shape[0]
    head_size = width // heads_here
    blocks = rows // SEG
    query_seg = queries.reshape(blocks, SEG, heads_here, head_size)
    key_seg = key_rows.reshape(blocks + LEFT, SEG, heads_here, head_size)
    value_seg = value_rows.reshape(blocks + LEFT, SEG, heads_here, head_size)
    live_seg = key_live.reshape(blocks + LEFT, SEG)
    key_band = jnp.concatenate(
        [key_seg[earlier : earlier + blocks] for earlier in range(LEFT + 1)], axis=1
    )
    value_band = jnp.concatenate(
        [value_seg[earlier : earlier + blocks] for earlier in range(LEFT + 1)], axis=1
    )
    live_band = jnp.concatenate(
        [live_seg[earlier : earlier + blocks] for earlier in range(LEFT + 1)], axis=1
    )
    scores = jnp.einsum("nqhd,nkhd->nhqk", query_seg, key_band, preferred_element_type=jnp.float32)
    scores = scores * head_size ** (-0.5) + bias[None]
    scores = jnp.where(live_band[:, None, None, :], scores, NEG_FILL)
    largest = jnp.max(scores, axis=-1, keepdims=True)
    weights = jnp.exp(scores - largest)
    weights = (weights / jnp.sum(weights, axis=-1, keepdims=True)).astype(jnp.bfloat16)
    mixed = jnp.einsum("nhqk,nkhd->nqhd", weights, value_band, preferred_element_type=jnp.float32)
    return mixed.astype(jnp.bfloat16).reshape(rows, width)


def extend_rows(pieces, member, own_rows):
    joined = jnp.concatenate([piece[member] for piece in pieces] + [own_rows], axis=0)
    return joined


def normed(hidden, gain):
    values = hidden.astype(jnp.float32)
    scale = lax.rsqrt(jnp.mean(values * values, axis=-1, keepdims=True) + EPS)
    return (values * scale * gain).astype(jnp.bfloat16)


def residual_add(branch, residual, gain):
    values = branch.astype(jnp.float32)
    scale = lax.rsqrt(jnp.mean(values * values, axis=-1, keepdims=True) + EPS)
    return (residual.astype(jnp.float32) + values * scale * gain).astype(jnp.bfloat16)


def combine(mixed, weight, residual, gain):
    partial_rows = jnp.dot(
        mixed, lax.all_gather(weight, "sp", axis=1, tiled=True), preferred_element_type=jnp.float32
    )
    branch = lax.psum_scatter(
        partial_rows.astype(jnp.bfloat16), "tp", scatter_dimension=0, tiled=True
    )
    return residual_add(branch, residual, gain)


def full_rows(share):
    return lax.all_gather(share, "tp", axis=0, tiled=True)


def shards(
    resid,
    queries_first,
    keys_first,
    values_first,
    rel_first,
    post_first,
    out_first,
    pre_second,
    query_weight,
    key_weight,
    value_weight,
    rel_second,
    post_second,
    out_second,
):
    tok_rows = resid.shape[0]
    n_sp = lax.axis_size("sp")
    if (
        rel_first.shape[0] == n_sp
        and n_sp % 2 == 0
        and lax.axis_size("tp") == 2
        and lax.axis_size("grp") == 2
        and REACH % tok_rows == 0
        and tok_rows == REL_CLIP
    ):
        return by_heads(
            resid, queries_first, keys_first, values_first, rel_first, post_first, out_first,
            pre_second, query_weight, key_weight, value_weight, rel_second, post_second, out_second,
        )
    depth = (REACH + tok_rows - 1) // tok_rows
    anchor = lax.axis_index("sp") * tok_rows
    key_live = anchor - REACH + jnp.arange(tok_rows + REACH, dtype=jnp.int32) >= 0
    share_rows = tok_rows // lax.axis_size("tp")
    base_rows = lax.dynamic_slice_in_dim(resid, lax.axis_index("tp") * share_rows, share_rows, 0)
    earlier_first = [
        from_behind((keys_first, values_first), "sp", distance) for distance in range(depth, 0, -1)
    ]
    key_ext = extend_rows(earlier_first, 0, keys_first)
    value_ext = extend_rows(earlier_first, 1, values_first)
    first = attend_band(queries_first, key_ext, value_ext, band_bias(rel_first), key_live)
    hidden_one = combine(first, out_first, base_rows, post_first)
    inputs_two = full_rows(normed(hidden_one, pre_second))
    query_sum = jnp.dot(
        inputs_two,
        lax.all_gather(query_weight, "sp", axis=0, tiled=True),
        preferred_element_type=jnp.float32,
    )
    key_sum = jnp.dot(
        inputs_two,
        lax.all_gather(key_weight, "sp", axis=0, tiled=True),
        preferred_element_type=jnp.float32,
    )
    value_sum = jnp.dot(
        inputs_two,
        lax.all_gather(value_weight, "sp", axis=0, tiled=True),
        preferred_element_type=jnp.float32,
    )
    queries_two = query_sum.astype(jnp.bfloat16)
    keys_two = key_sum.astype(jnp.bfloat16)
    values_two = value_sum.astype(jnp.bfloat16)
    earlier_second = [
        from_behind((keys_two, values_two), "sp", distance) for distance in range(depth, 0, -1)
    ]
    key_ext_two = extend_rows(earlier_second, 0, keys_two)
    value_ext_two = extend_rows(earlier_second, 1, values_two)
    second = attend_band(queries_two, key_ext_two, value_ext_two, band_bias(rel_second), key_live)
    hidden_two = combine(second, out_second, hidden_one, post_second)
    return full_rows(hidden_two)


def scaled(values):
    return values * lax.rsqrt(jnp.mean(values * values, axis=-1, keepdims=True) + EPS)


def build_kernel(n, tok, head, width, reach):
    share = tok // 2
    cols = width // n
    span = reach + tok
    levels = n // 2
    depth = n * head
    dhalf = depth // 2
    wrows = width // n
    hrows = wrows // 2
    pieces = 4
    cuts = 2
    wide = width // pieces

    def kernel(
        q_hbm, k_hbm, v_hbm, wq_hbm, wk_hbm, wv_hbm, resid_hbm, o1_hbm, o2_hbm,
        rel1_hbm, rel2_hbm, post1_hbm, pre2_hbm, post2_hbm,
        out_ref,
        heads, weights, outs, res, bias, own_mix, mixed, parts, inbox, joined, branch, rows2,
        rel1, rel2, post1, pre2, post2,
        loc_sem, hs, hr, ws, wr, wf, wh, mzs, mzr, mys, myr, ozs, ozr, oxs, oxr,
        ms, mr, ns, nr, nxs, nxr, ps, pr, bs, br, rzs, rzr, rys, ryr, rds, rdr, fs, fr,
    ):
        s = lax.axis_index("sp")
        t = lax.axis_index("tp")
        g = lax.axis_index("grp")
        u = 1 - t
        z = s // 2
        y = lax.rem(s, 2)
        v = 1 - y
        side = 2 * z + v
        turn = 1 - 2 * lax.rem(z, 2)
        rung = lax.rem(z, 2)
        twin = z + 1 - 2 * rung
        across = lax.rem(z + levels // 2, levels)

        def rcopy(src, dst, ssem, rsem, sp, tp, grp=g):
            return pltpu.make_async_remote_copy(
                src_ref=src, dst_ref=dst, send_sem=ssem, recv_sem=rsem,
                device_id={"grp": grp, "sp": sp, "tp": tp}, device_id_type=MESH,
            )

        def peer(k):
            return lax.rem(s + k, n)

        def near_level(i):
            return lax.rem(z + turn * i + levels, levels)

        def by_distance(i):
            low = jnp.minimum(z, levels - 1 - z)
            c = jnp.where(i <= low, low - i, i)
            return jnp.where(2 * z < levels, c, levels - 1 - c)

        def arrived(ref, sem):
            pltpu.make_async_copy(ref, ref, sem).wait()

        small = [
            pltpu.make_async_copy(src, dst, loc_sem.at[3 + i])
            for i, (src, dst) in enumerate(
                ((rel1_hbm, rel1), (rel2_hbm, rel2), (post1_hbm, post1), (pre2_hbm, pre2),
                 (post2_hbm, post2))
            )
        ]
        for copy in small:
            copy.start()

        barrier = pltpu.get_barrier_semaphore()
        for k in range(1, n):
            pl.semaphore_signal(
                barrier, inc=1, device_id={"grp": g, "sp": peer(k), "tp": t}, device_id_type=MESH
            )
        pl.semaphore_signal(
            barrier, inc=1, device_id={"grp": g, "sp": s, "tp": u}, device_id_type=MESH
        )
        pl.semaphore_signal(
            barrier, inc=1, device_id={"grp": 1 - g, "sp": s, "tp": t}, device_id_type=MESH
        )
        pl.semaphore_wait(barrier, n + 1)

        def lanes(j):
            return pl.ds(pl.multiple_of(j * head, head), head)

        def trows(j, base=0):
            return pl.ds(pl.multiple_of(base + j * tok, tok), tok)

        def close(k):
            return jnp.where(k == 0, side, jnp.where(k == 1, 2 * twin + y, 2 * twin + v))

        def distant(k):
            level = across + lax.rem(k // 2, 2) * (1 - 2 * lax.rem(across, 2))
            return 2 * level + lax.rem(y + k, 2)

        qkv = (q_hbm, k_hbm, v_hbm)
        wqkv = (wq_hbm, wk_hbm, wv_hbm)

        def head_copy(i, j):
            dst = heads.at[i, trows(s, reach)]
            return rcopy(qkv[i].at[:, lanes(j)], dst, hs, hr.at[s], j, t)

        def weight_half(src, part):
            start = pl.multiple_of(src * wrows + part * hrows, hrows)
            return weights.at[pl.ds(start, hrows)]

        def weight_copy(i, j):
            start = pl.multiple_of(s * wrows + g * hrows, hrows)
            piece = wqkv[i].at[pl.ds(pl.multiple_of(g * hrows, hrows), hrows), lanes(j)]
            dst = weights.at[pl.ds(start, hrows), pl.ds(i * head, head)]
            return rcopy(piece, dst, ws, wr.at[s], j, t)

        def weight_hand(src):
            piece = weight_half(src, g)
            return rcopy(piece, piece, wf, wh, s, t, 1 - g)

        dcut = dhalf // cuts

        def out_half(c, part):
            return outs.at[0, c, pl.ds(pl.multiple_of(part * dhalf, dhalf), dhalf)]

        def out_piece(c, h):
            return outs.at[0, c, pl.ds(pl.multiple_of(g * dhalf + h * dcut, dcut), dcut)]

        def out_own(h, to):
            piece = o1_hbm.at[pl.ds(pl.multiple_of(g * dhalf + h * dcut, dcut), dcut)]
            return rcopy(piece, out_piece(z, h), ozs, ozr.at[z, h], 2 * to + y, t)

        def out_pass(c, h, to):
            piece = out_piece(c, h)
            return rcopy(piece, piece, ozs, ozr.at[c, h], 2 * to + y, t)

        def out_hand(c, h):
            piece = out_piece(c, h)
            return rcopy(piece, piece, oxs, oxr.at[c], s, t, 1 - g)

        def out_start():
            for h in range(cuts):
                @pl.when(z < levels - 1)
                def _():
                    out_own(h, z + 1).start()

                @pl.when(z > 0)
                def _():
                    out_own(h, z - 1).start()

        def out_hop(d):
            for h in range(cuts):
                @pl.when(z >= d)
                def _():
                    arrived(out_piece(z - d, h), ozr.at[z - d, h])

                    @pl.when(z < levels - 1)
                    def _():
                        out_pass(z - d, h, z + 1).start()

                    out_hand(z - d, h).start()

                @pl.when(z + d < levels)
                def _():
                    arrived(out_piece(z + d, h), ozr.at[z + d, h])

                    @pl.when(z > 0)
                    def _():
                        out_pass(z + d, h, z - 1).start()

                    out_hand(z + d, h).start()

        def two_half(e, part):
            return outs.at[1, e, pl.ds(pl.multiple_of(part * dhalf, dhalf), dhalf)]

        def two_own(e, sp):
            piece = o2_hbm.at[pl.ds(pl.multiple_of(g * dhalf, dhalf), dhalf)]
            return rcopy(piece, two_half(e, g), ns, nr.at[e], sp, t)

        def two_side():
            piece = two_half(2 + y, g)
            return rcopy(piece, piece, ns, nr.at[2 + y], side, t)

        def two_hand(e):
            piece = two_half(e, g)
            return rcopy(piece, piece, nxs, nxr.at[e], s, t, 1 - g)

        def two_start():
            two_own(2 + y, 2 * across + y).start()

        def two_near():
            arrived(two_half(2 + y, g), nr.at[2 + y])
            two_side().start()
            two_hand(2 + y).start()

        def two_far():
            arrived(two_half(2 + v, g), nr.at[2 + v])
            two_hand(2 + v).start()

        def out_drain():
            for at in range(levels):
                count = (1 + at if at < levels - 1 else 0) + (levels - at if at > 0 else 0)
                block = rows2.at[pl.ds(0, count)]

                @pl.when(z == at)
                def _():
                    arrived(block, ozs)

            arrived(rows2.at[pl.ds(0, levels - 1)], oxs)

        out_start()
        for i in range(3):
            head_copy(i, side).start()
        for a in range(1, levels):
            for j in (y, v):
                for i in range(3):
                    head_copy(i, 2 * by_distance(a) + j).start()
        for i in range(3):
            pltpu.make_async_copy(
                qkv[i].at[:, lanes(s)], heads.at[i, trows(s, reach)], hr.at[s]
            ).start()
        for i in range(3):
            pltpu.make_async_copy(
                wqkv[i].at[:, lanes(s)],
                weights.at[pl.ds(pl.multiple_of(s * wrows, wrows), wrows), pl.ds(i * head, head)],
                wr.at[s],
            ).start()
        two_own(y, side).start()
        for k in range(0, 3):
            for i in range(3):
                weight_copy(i, close(k)).start()
        local = [
            pltpu.make_async_copy(o1_hbm, outs.at[0, z], loc_sem.at[0]),
            pltpu.make_async_copy(o2_hbm, outs.at[1, y], loc_sem.at[1]),
            pltpu.make_async_copy(
                resid_hbm.at[pl.ds(pl.multiple_of(t * share, share), share)], res, loc_sem.at[2]
            ),
        ]
        for copy in local:
            copy.start()

        for copy in small:
            copy.wait()
        near = 2 * REL_CLIP
        query = lax.broadcasted_iota(jnp.int32, (tok, span), 0) // SEG
        key = lax.broadcasted_iota(jnp.int32, (tok, span), 1) // SEG
        live = (key >= query) & (key <= query + LEFT)
        for layer, rel in enumerate((rel1, rel2)):
            table = rel[pl.ds(s, 1), :]
            top = table[:, near : near + 1]
            entry = lax.broadcasted_iota(jnp.int32, (near, near + tok), 0)
            place = lax.broadcasted_iota(jnp.int32, (near, near + tok), 1)
            flip = (entry + place == near).astype(F32)
            line = jnp.dot(
                jnp.broadcast_to(table[:, :near], (8, near)), flip,
                preferred_element_type=F32, precision=lax.Precision.HIGHEST,
            )[:1]
            spot = lax.broadcasted_iota(jnp.int32, line.shape, 1)
            line = jnp.where((spot == 0) | (spot >= near), top, line)
            spread = jnp.broadcast_to(line, (tok, near + tok))
            row = lax.broadcasted_iota(jnp.int32, spread.shape, 0)
            step = 1
            while step < tok:
                moved = pltpu.roll(spread, step, 1)
                spread = jnp.where(lax.rem(row // step, 2) == 1, moved, spread)
                step *= 2
            far = jnp.broadcast_to(top, (tok, span - near))
            whole = jnp.concatenate([far, spread[:, :near]], axis=1)
            bias[layer] = jnp.where(live, whole, NEG_FILL)

        heads[1, :reach] = jnp.zeros((reach, head), BF16)
        heads[2, :reach] = jnp.zeros((reach, head), BF16)

        def attend(layer, b):
            qb = heads[0, trows(b, reach)]
            kb = heads[1, pl.ds(pl.multiple_of(b * tok, tok), span)]
            vb = heads[2, pl.ds(pl.multiple_of(b * tok, tok), span)]
            scores = lax.dot_general(
                qb, kb, (((1,), (1,)), ((), ())), preferred_element_type=F32
            ) * head ** (-0.5) + bias[layer]
            column = lax.broadcasted_iota(jnp.int32, scores.shape, 1)
            scores = jnp.where(column >= reach - b * tok, scores, NEG_FILL)
            e = jnp.exp(scores - jnp.max(scores, axis=-1, keepdims=True))
            e = (e * (1.0 / jnp.sum(e, axis=-1, keepdims=True))).astype(BF16)
            return jnp.dot(e, vb, preferred_element_type=F32).astype(BF16)

        def mix_z(layer, b):
            dst = mixed.at[layer, s, trows(lax.rem(b, 2))]
            return rcopy(
                own_mix.at[layer, b], dst, mzs.at[layer], mzr.at[layer, z], 2 * (b // 2) + y, t
            )

        def mix_y(layer, c):
            block = mixed.at[layer, 2 * c + y]
            return rcopy(block, block, mys.at[layer], myr.at[layer, c], side, t)

        def one_head(layer, order, wait_block):
            def one(i, _):
                b = order(i)
                wait_block(b)
                result = attend(layer, b)

                @pl.when(b // 2 != z)
                def _():
                    own_mix[layer, b] = result
                    mix_z(layer, b).start()

                @pl.when(b // 2 == z)
                def _():
                    mixed[layer, s, trows(lax.rem(b, 2))] = result

                    @pl.when(lax.rem(b, 2) == 1)
                    def _():
                        mix_y(layer, z).start()

                return 0

            return one

        def forward_mix(layer):
            def one(i, _):
                c = near_level(i)
                arrived(mixed.at[layer, 2 * c + y], mzr.at[layer, c])
                mix_y(layer, c).start()
                return 0

            lax.fori_loop(1, levels, one, 0)

        def two_copy(layer, b, level):
            dst = mixed.at[layer, s, trows(lax.rem(b // 2, 2))]
            return rcopy(
                own_mix.at[layer, b], dst, ms, mr,
                2 * level + lax.rem(b, 2), t,
            )

        def two_head(layer, order, wait_block):
            def one(i, _):
                b = order(i)
                wait_block(b)
                result = attend(layer, b)
                own_mix[layer, b] = result
                level = b // 2
                other = level + 1 - 2 * lax.rem(level, 2)
                mine = lax.rem(b, 2) == y

                @pl.when(jnp.logical_not(mine & (level == z)))
                def _():
                    two_copy(layer, b, level).start()

                @pl.when(jnp.logical_not(mine & (other == z)))
                def _():
                    two_copy(layer, b, other).start()

                @pl.when(mine & (level // 2 == z // 2))
                def _():
                    mixed[layer, s, trows(lax.rem(level, 2))] = result

                return 0

            return one

        def pcopy(layer, c):
            return rcopy(
                parts.at[layer, c, u], inbox.at[layer, c],
                ps.at[layer], pr.at[layer, c], s, u,
            )

        def bcopy(layer, c):
            if layer == 0:
                return rcopy(
                    joined.at[layer, c, v], branch.at[layer, y, c], bs.at[layer], br.at[layer],
                    side, t,
                )
            return rcopy(
                joined.at[layer, c, 1 - rung], branch.at[layer, rung, c],
                bs.at[layer], br.at[layer], 2 * twin + y, t,
            )

        def project_branch(layer):
            if layer == 0:
                for c in range(levels):
                    arrived(mixed.at[layer, 2 * c + v], myr.at[layer, c])
                own_block, mine, order = z, y, near_level
                hand_ready = lambda c: arrived(out_half(c, 1 - g), oxr.at[c])
            else:
                arrived(mixed.at[layer, pl.ds(0, n - 1)], mr)
                own_block, mine = y, rung
                order = lambda i: 2 * (i // 2) + lax.rem(y + i, 2)
                hand_ready = lambda e: arrived(two_half(e, 1 - g), nxr.at[e])
            local[layer].wait()

            def project(c):
                @pl.when(c != own_block)
                def _():
                    hand_ready(c)

                lhs = jnp.concatenate([mixed[layer, j] for j in range(n)], axis=1)
                part = jnp.dot(lhs, outs[layer, c], preferred_element_type=F32).astype(BF16)
                for p in range(2):
                    for q in range(2):
                        parts[layer, c, q, p] = part[p * tok + q * share : p * tok + (q + 1) * share]
                pcopy(layer, c).start()

            def join(c):
                arrived(inbox.at[layer, c], pr.at[layer, c])
                both = parts[layer, c, t].astype(F32) + inbox[layer, c].astype(F32)
                joined[layer, c] = both.astype(BF16)
                bcopy(layer, c).start()
                branch[layer, mine, c] = joined[layer, c, mine]

            def step(i, _):
                project(order(i))

                @pl.when(i > 0)
                def _():
                    join(order(i - 1))

                return 0

            lax.fori_loop(0, levels, step, 0)
            join(order(levels - 1))
            arrived(branch.at[layer, 1 - mine], br.at[layer])

            def column_block(j):
                if layer == 0:
                    return branch[layer, j % 2, j // 2]
                half = lax.rem(j // levels + 2 * z // levels, 2)
                return branch[layer, (j // 2) % 2, 2 * half + j % 2]

            values = jnp.concatenate([column_block(j) for j in range(n)], axis=1)
            return values.astype(F32)

        def branch_drain(layer):
            if layer == 0:
                arrived(own_mix.at[layer, pl.ds(0, n - 2)], mzs.at[layer])
                arrived(mixed.at[layer, pl.ds(0, levels)], mys.at[layer])
            else:
                arrived(mixed.at[layer, pl.ds(0, n - 1)], ms)
            arrived(inbox.at[layer], ps.at[layer])
            arrived(branch.at[layer, 0], bs.at[layer])

        def hand_weights(src):
            arrived(weight_half(src, g), wr.at[src])
            weight_hand(src).start()
            return 0

        def heads_ready(b):
            arrived(heads.at[:, trows(b, reach)], hr.at[b])

        out_hop(1)
        lax.fori_loop(0, n, one_head(0, lambda i: i, heads_ready), 0)
        out_hop(2)
        forward_mix(0)
        for k in range(0, 4):
            for i in range(3):
                weight_copy(i, distant(k)).start()
        for d in range(3, levels):
            out_hop(d)
        lax.fori_loop(0, 3, lambda k, c: hand_weights(close(k)), 0)
        values = project_branch(0)
        local[2].wait()
        hidden = (res[...].astype(F32) + scaled(values) * post1[...]).astype(BF16)
        res[...] = hidden
        rows2[2 * s + t] = (scaled(hidden.astype(F32)) * pre2[...]).astype(BF16)

        def piece_of(item, m):
            return rows2.at[item, :, pl.ds(pl.multiple_of(m * wide, wide), wide)]

        def row_z(c, m, to):
            block = piece_of(2 * (2 * c + y) + t, m)
            return rcopy(block, block, rzs, rzr.at[c, m], 2 * to + y, t)

        def row_y(c, m):
            block = piece_of(2 * (2 * c + y) + t, m)
            return rcopy(block, block, rys, ryr.at[c, m], side, t)

        def row_d(src, m):
            block = piece_of(2 * src + t, m)
            return rcopy(block, block, rds, rdr.at[src // 2], s, u)

        def own_rows(m, _):
            @pl.when(z < levels - 1)
            def _():
                row_z(z, m, z + 1).start()

            @pl.when(z > 0)
            def _():
                row_z(z, m, z - 1).start()

            row_y(z, m).start()
            row_d(s, m).start()
            return 0

        lax.fori_loop(0, pieces, own_rows, 0)
        two_start()

        lax.fori_loop(0, 4, lambda k, c: hand_weights(distant(k)), 0)
        arrived(two_half(v, g), nr.at[v])
        two_hand(v).start()

        def from_level(c, m, on, to):
            arrived(piece_of(2 * (2 * c + y) + t, m), rzr.at[c, m])

            @pl.when(on)
            def _():
                row_z(c, m, to).start()

            row_y(c, m).start()
            row_d(2 * c + y, m).start()

        def from_side(c, m):
            arrived(piece_of(2 * (2 * c + v) + t, m), ryr.at[c, m])
            row_d(2 * c + v, m).start()

        def rows_hop(d):
            def one(m, _):
                if d < levels:
                    @pl.when(z >= d)
                    def _():
                        from_level(z - d, m, z < levels - 1, z + 1)

                    @pl.when(z + d < levels)
                    def _():
                        from_level(z + d, m, z > 0, z - 1)

                if d == 1:
                    from_side(z, m)
                else:
                    @pl.when(z >= d - 1)
                    def _():
                        from_side(z - (d - 1), m)

                    @pl.when(z + d - 1 < levels)
                    def _():
                        from_side(z + (d - 1), m)

                return 0

            lax.fori_loop(0, pieces, one, 0)

        def project_rows(i, _):
            c = by_distance(i)
            arrived(rows2.at[pl.ds(4 * c, 2)], rdr.at[c])
            lhs = rows2[pl.ds(4 * c, 4)].reshape(2 * tok, width)
            both = jnp.dot(lhs, weights[...], preferred_element_type=F32).astype(BF16)
            start = pl.ds(pl.multiple_of(reach + c * 2 * tok, tok), 2 * tok)
            for i in range(3):
                heads[i, start] = both[:, i * head : (i + 1) * head]
            return 0

        def weights_here():
            arrived(weights.at[pl.ds(0, (n - 1) * hrows)], wh)
            arrived(weights.at[pl.ds(pl.multiple_of(s * wrows, wrows), wrows)], wr.at[s])

        lag = reach // tok
        top = z == levels - 1
        early = jnp.where(top, n - 2 - lag, jnp.where(z == 0, n - 2, n))
        begin = jnp.where(top, lag + 2, jnp.where(2 * z < levels, lag, 0))

        def two_order(i):
            first = lax.rem(lag + i, n - 2)
            return jnp.where(z == 0, jnp.where(i < n - 2, first, i), lax.rem(begin + i, n))

        known = jnp.where(top | (z == 0), levels - 1, levels)
        head_two = two_head(1, two_order, lambda b: None)

        for d in range(1, levels + 1):
            rows_hop(d)
            if d == 2:
                weights_here()
                lax.fori_loop(0, 2, project_rows, 0)
            if d == levels - 1:
                two_near()
                lax.fori_loop(2, known, project_rows, 0)
                lax.fori_loop(0, early, head_two, 0)
        lax.fori_loop(known, levels, project_rows, 0)
        lax.fori_loop(early, n, head_two, 0)
        two_far()
        values = project_branch(1)
        done = (res[...].astype(F32) + scaled(values) * post2[...]).astype(BF16)
        mine_rows = out_ref.at[pl.ds(pl.multiple_of(t * share, share), share)]
        mine_rows[...] = done
        final = rcopy(mine_rows, mine_rows, fs, fr, s, u)
        final.start()

        arrived(heads.at[:, pl.ds(reach, (n - 1) * tok)], hs)
        arrived(weights.at[pl.ds(0, (n - 1) * hrows)], ws)
        arrived(weights.at[pl.ds(0, (n - 1) * hrows)], wf)
        out_drain()
        arrived(rows2.at[pl.ds(0, 3)], ns)
        arrived(rows2.at[pl.ds(0, 3)], nxs)
        for layer in range(2):
            branch_drain(layer)
        for at in range(levels):
            count = (1 + at if at < levels - 1 else 0) + (levels - at if at > 0 else 0)
            block = rows2.at[pl.ds(0, count)]

            @pl.when(z == at)
            def _():
                arrived(block, rzs)

        arrived(rows2.at[pl.ds(0, levels)], rys)
        arrived(rows2.at[pl.ds(0, n)], rds)
        final.wait_send()
        other_rows = out_ref.at[pl.ds(pl.multiple_of(u * share, share), share)]
        rcopy(other_rows, other_rows, fs, fr, s, u).wait_recv()

    dma = pltpu.SemaphoreType.DMA
    scratch = [
        pltpu.VMEM((3, reach + n * tok, head), BF16),
        pltpu.VMEM((width, 3 * head), BF16),
        pltpu.VMEM((2, levels, depth, cols), BF16),
        pltpu.VMEM((share, width), BF16),
        pltpu.VMEM((2, tok, span), F32),
        pltpu.VMEM((2, n, tok, head), BF16),
        pltpu.VMEM((2, n, 2 * tok, head), BF16),
        pltpu.VMEM((2, levels, 2, 2, share, cols), BF16),
        pltpu.VMEM((2, levels, 2, share, cols), BF16),
        pltpu.VMEM((2, levels, 2, share, cols), BF16),
        pltpu.VMEM((2, 2, levels, share, cols), BF16),
        pltpu.VMEM((2 * n, share, width), BF16),
        pltpu.VMEM((n, 2 * REL_CLIP + 1), F32),
        pltpu.VMEM((n, 2 * REL_CLIP + 1), F32),
        pltpu.VMEM((1, width), F32),
        pltpu.VMEM((1, width), F32),
        pltpu.VMEM((1, width), F32),
        dma((8,)),
        dma, dma((n,)),
        dma, dma((n,)), dma, dma,
        dma((1,)), dma((1, levels)), dma((1,)), dma((1, levels)),
        dma, dma((levels, cuts)), dma, dma((levels,)),
        dma, dma, dma, dma((levels,)), dma, dma((levels,)),
        dma((2,)), dma((2, levels)), dma((2,)), dma((2,)),
        dma, dma((levels, pieces)), dma, dma((levels, pieces)), dma, dma((levels,)),
        dma, dma,
    ]
    return kernel, scratch


def by_heads(
    resid, queries_first, keys_first, values_first, rel_first, post_first, out_first, pre_second,
    query_weight, key_weight, value_weight, rel_second, post_second, out_second,
):
    n = lax.axis_size("sp")
    tok, width = resid.shape
    head = queries_first.shape[1] // rel_first.shape[0]
    kernel, scratch = build_kernel(n, tok, head, width, REACH)
    hbm = pl.BlockSpec(memory_space=pltpu.HBM)
    vmem = pl.BlockSpec(memory_space=pltpu.VMEM)
    return pl.pallas_call(
        kernel,
        out_shape=pltpu.VMEM((tok, width), BF16),
        in_specs=[hbm] * 14,
        out_specs=vmem,
        scratch_shapes=scratch,
        compiler_params=pltpu.CompilerParams(
            collective_id=0, has_side_effects=True, vmem_limit_bytes=60 * 2**20
        ),
    )(
        queries_first, keys_first, values_first, query_weight, key_weight, value_weight, resid,
        out_first, out_second, rel_first, rel_second,
        post_first[None], pre_second[None], post_second[None],
    )


def solution(mesh):
    in_specs = (
        P(("grp", "sp"), None),
        P(("grp", "sp"), "tp"),
        P(("grp", "sp"), "tp"),
        P(("grp", "sp"), "tp"),
        P("tp", None),
        P(),
        P("tp", "sp"),
        P(),
        P("sp", "tp"),
        P("sp", "tp"),
        P("sp", "tp"),
        P("tp", None),
        P(),
        P("tp", "sp"),
    )
    out_specs = P(("grp", "sp"), None)
    return jax.shard_map(shards, mesh=mesh, in_specs=in_specs, out_specs=out_specs, check_vma=False)
```

```python
import jax
import jax.numpy as jnp
from jax import lax
from jax.experimental import pallas as pl
from jax.experimental.pallas import tpu as pltpu
from jax.sharding import PartitionSpec as P

MESH = pl.DeviceIdType.MESH
BF16 = jnp.bfloat16
F32 = jnp.float32

SEG = 64
LEFT = 8
REACH = 512
REL_CLIP = 128


EPS = 1e-06
NEG_FILL = -1e30


def from_behind(value, axis, steps):
    count = lax.axis_size(axis)
    initial, last = (max(0, -steps), min(count, count - steps))
    return lax.ppermute(value, axis, [(source, source + steps) for source in range(initial, last)])


def band_bias(bias_table):
    heads_here = bias_table.shape[0]
    band = (LEFT + 1) * SEG
    length = SEG + band
    index = jnp.arange(length, dtype=jnp.int32)
    distance = jnp.where(index < band, LEFT * SEG - index, LEFT * SEG + length - index)
    slot = jnp.clip(distance, -REL_CLIP, REL_CLIP) + REL_CLIP
    onehot = (slot[:, None] == jnp.arange(2 * REL_CLIP + 1, dtype=jnp.int32)[None, :]).astype(
        jnp.float32
    )
    diagonal_values = jnp.dot(bias_table, onehot.T, precision=lax.Precision.HIGHEST)
    spread = jnp.broadcast_to(diagonal_values[:, None, :], (heads_here, SEG, length)).reshape(
        heads_here, SEG * length
    )
    return spread[:, : SEG * (length - 1)].reshape(heads_here, SEG, length - 1)[:, :, :band]


def attend_band(queries, key_rows, value_rows, bias, key_live):
    rows, width = queries.shape
    heads_here = bias.shape[0]
    head_size = width // heads_here
    blocks = rows // SEG
    query_seg = queries.reshape(blocks, SEG, heads_here, head_size)
    key_seg = key_rows.reshape(blocks + LEFT, SEG, heads_here, head_size)
    value_seg = value_rows.reshape(blocks + LEFT, SEG, heads_here, head_size)
    live_seg = key_live.reshape(blocks + LEFT, SEG)
    key_band = jnp.concatenate(
        [key_seg[earlier : earlier + blocks] for earlier in range(LEFT + 1)], axis=1
    )
    value_band = jnp.concatenate(
        [value_seg[earlier : earlier + blocks] for earlier in range(LEFT + 1)], axis=1
    )
    live_band = jnp.concatenate(
        [live_seg[earlier : earlier + blocks] for earlier in range(LEFT + 1)], axis=1
    )
    scores = jnp.einsum("nqhd,nkhd->nhqk", query_seg, key_band, preferred_element_type=jnp.float32)
    scores = scores * head_size ** (-0.5) + bias[None]
    scores = jnp.where(live_band[:, None, None, :], scores, NEG_FILL)
    largest = jnp.max(scores, axis=-1, keepdims=True)
    weights = jnp.exp(scores - largest)
    weights = (weights / jnp.sum(weights, axis=-1, keepdims=True)).astype(jnp.bfloat16)
    mixed = jnp.einsum("nhqk,nkhd->nqhd", weights, value_band, preferred_element_type=jnp.float32)
    return mixed.astype(jnp.bfloat16).reshape(rows, width)


def extend_rows(pieces, member, own_rows):
    joined = jnp.concatenate([piece[member] for piece in pieces] + [own_rows], axis=0)
    return joined


def normed(hidden, gain):
    values = hidden.astype(jnp.float32)
    scale = lax.rsqrt(jnp.mean(values * values, axis=-1, keepdims=True) + EPS)
    return (values * scale * gain).astype(jnp.bfloat16)


def residual_add(branch, residual, gain):
    values = branch.astype(jnp.float32)
    scale = lax.rsqrt(jnp.mean(values * values, axis=-1, keepdims=True) + EPS)
    return (residual.astype(jnp.float32) + values * scale * gain).astype(jnp.bfloat16)


def combine(mixed, weight, residual, gain):
    partial_rows = jnp.dot(
        mixed, lax.all_gather(weight, "sp", axis=1, tiled=True), preferred_element_type=jnp.float32
    )
    branch = lax.psum_scatter(
        partial_rows.astype(jnp.bfloat16), "tp", scatter_dimension=0, tiled=True
    )
    return residual_add(branch, residual, gain)


def full_rows(share):
    return lax.all_gather(share, "tp", axis=0, tiled=True)


def shards(
    resid,
    queries_first,
    keys_first,
    values_first,
    rel_first,
    post_first,
    out_first,
    pre_second,
    query_weight,
    key_weight,
    value_weight,
    rel_second,
    post_second,
    out_second,
):
    tok_rows = resid.shape[0]
    n_sp = lax.axis_size("sp")
    if (
        rel_first.shape[0] == n_sp
        and n_sp % 2 == 0
        and lax.axis_size("tp") == 2
        and lax.axis_size("grp") == 2
        and REACH % tok_rows == 0
        and tok_rows == REL_CLIP
    ):
        return by_heads(
            resid, queries_first, keys_first, values_first, rel_first, post_first, out_first,
            pre_second, query_weight, key_weight, value_weight, rel_second, post_second, out_second,
        )
    depth = (REACH + tok_rows - 1) // tok_rows
    anchor = lax.axis_index("sp") * tok_rows
    key_live = anchor - REACH + jnp.arange(tok_rows + REACH, dtype=jnp.int32) >= 0
    share_rows = tok_rows // lax.axis_size("tp")
    base_rows = lax.dynamic_slice_in_dim(resid, lax.axis_index("tp") * share_rows, share_rows, 0)
    earlier_first = [
        from_behind((keys_first, values_first), "sp", distance) for distance in range(depth, 0, -1)
    ]
    key_ext = extend_rows(earlier_first, 0, keys_first)
    value_ext = extend_rows(earlier_first, 1, values_first)
    first = attend_band(queries_first, key_ext, value_ext, band_bias(rel_first), key_live)
    hidden_one = combine(first, out_first, base_rows, post_first)
    inputs_two = full_rows(normed(hidden_one, pre_second))
    query_sum = jnp.dot(
        inputs_two,
        lax.all_gather(query_weight, "sp", axis=0, tiled=True),
        preferred_element_type=jnp.float32,
    )
    key_sum = jnp.dot(
        inputs_two,
        lax.all_gather(key_weight, "sp", axis=0, tiled=True),
        preferred_element_type=jnp.float32,
    )
    value_sum = jnp.dot(
        inputs_two,
        lax.all_gather(value_weight, "sp", axis=0, tiled=True),
        preferred_element_type=jnp.float32,
    )
    queries_two = query_sum.astype(jnp.bfloat16)
    keys_two = key_sum.astype(jnp.bfloat16)
    values_two = value_sum.astype(jnp.bfloat16)
    earlier_second = [
        from_behind((keys_two, values_two), "sp", distance) for distance in range(depth, 0, -1)
    ]
    key_ext_two = extend_rows(earlier_second, 0, keys_two)
    value_ext_two = extend_rows(earlier_second, 1, values_two)
    second = attend_band(queries_two, key_ext_two, value_ext_two, band_bias(rel_second), key_live)
    hidden_two = combine(second, out_second, hidden_one, post_second)
    return full_rows(hidden_two)


def scaled(values):
    return values * lax.rsqrt(jnp.mean(values * values, axis=-1, keepdims=True) + EPS)


def build_kernel(n, tok, head, width, reach):
    share = tok // 2
    cols = width // n
    span = reach + tok
    levels = n // 2
    depth = n * head
    dhalf = depth // 2
    wrows = width // n
    hrows = wrows // 2
    pieces = 4
    cuts = 2
    wide = width // pieces

    def kernel(
        q_hbm, k_hbm, v_hbm, wq_hbm, wk_hbm, wv_hbm, resid_hbm, o1_hbm, o2_hbm,
        rel1_hbm, rel2_hbm, post1_hbm, pre2_hbm, post2_hbm,
        out_ref,
        heads, weights, outs, res, bias, own_mix, mixed, parts, inbox, joined, branch, rows2,
        rel1, rel2, post1, pre2, post2,
        loc_sem, hs, hr, ws, wr, wf, wh, mzs, mzr, mys, myr, ozs, ozr, oxs, oxr,
        ms, mr, ns, nr, nxs, nxr, ps, pr, bs, br, rzs, rzr, rys, ryr, rds, rdr, fs, fr,
    ):
        s = lax.axis_index("sp")
        t = lax.axis_index("tp")
        g = lax.axis_index("grp")
        u = 1 - t
        z = s // 2
        y = lax.rem(s, 2)
        v = 1 - y
        side = 2 * z + v
        turn = 1 - 2 * lax.rem(z, 2)
        rung = lax.rem(z, 2)
        twin = z + 1 - 2 * rung
        across = lax.rem(z + levels // 2, levels)

        def rcopy(src, dst, ssem, rsem, sp, tp, grp=g):
            return pltpu.make_async_remote_copy(
                src_ref=src, dst_ref=dst, send_sem=ssem, recv_sem=rsem,
                device_id={"grp": grp, "sp": sp, "tp": tp}, device_id_type=MESH,
            )

        def peer(k):
            return lax.rem(s + k, n)

        def near_level(i):
            return lax.rem(z + turn * i + levels, levels)

        def by_distance(i):
            low = jnp.minimum(z, levels - 1 - z)
            c = jnp.where(i <= low, low - i, i)
            return jnp.where(2 * z < levels, c, levels - 1 - c)

        def arrived(ref, sem):
            pltpu.make_async_copy(ref, ref, sem).wait()

        small = [
            pltpu.make_async_copy(src, dst, loc_sem.at[3 + i])
            for i, (src, dst) in enumerate(
                ((rel1_hbm, rel1), (rel2_hbm, rel2), (post1_hbm, post1), (pre2_hbm, pre2),
                 (post2_hbm, post2))
            )
        ]
        for copy in small:
            copy.start()

        barrier = pltpu.get_barrier_semaphore()
        for k in range(1, n):
            pl.semaphore_signal(
                barrier, inc=1, device_id={"grp": g, "sp": peer(k), "tp": t}, device_id_type=MESH
            )
        pl.semaphore_signal(
            barrier, inc=1, device_id={"grp": g, "sp": s, "tp": u}, device_id_type=MESH
        )
        pl.semaphore_signal(
            barrier, inc=1, device_id={"grp": 1 - g, "sp": s, "tp": t}, device_id_type=MESH
        )
        pl.semaphore_wait(barrier, n + 1)

        def lanes(j):
            return pl.ds(pl.multiple_of(j * head, head), head)

        def trows(j, base=0):
            return pl.ds(pl.multiple_of(base + j * tok, tok), tok)

        def close(k):
            return jnp.where(k == 0, side, jnp.where(k == 1, 2 * twin + y, 2 * twin + v))

        def distant(k):
            level = across + lax.rem(k // 2, 2) * (1 - 2 * lax.rem(across, 2))
            return 2 * level + lax.rem(y + k, 2)

        qkv = (q_hbm, k_hbm, v_hbm)
        wqkv = (wq_hbm, wk_hbm, wv_hbm)

        def head_copy(i, j):
            dst = heads.at[i, trows(s, reach)]
            return rcopy(qkv[i].at[:, lanes(j)], dst, hs, hr.at[s], j, t)

        def weight_half(src, part):
            start = pl.multiple_of(src * wrows + part * hrows, hrows)
            return weights.at[pl.ds(start, hrows)]

        def weight_copy(i, j):
            start = pl.multiple_of(s * wrows + g * hrows, hrows)
            piece = wqkv[i].at[pl.ds(pl.multiple_of(g * hrows, hrows), hrows), lanes(j)]
            dst = weights.at[pl.ds(start, hrows), pl.ds(i * head, head)]
            return rcopy(piece, dst, ws, wr.at[s], j, t)

        def weight_hand(src):
            piece = weight_half(src, g)
            return rcopy(piece, piece, wf, wh, s, t, 1 - g)

        dcut = dhalf // cuts

        def out_half(c, part):
            return outs.at[0, c, pl.ds(pl.multiple_of(part * dhalf, dhalf), dhalf)]

        def out_piece(c, h):
            return outs.at[0, c, pl.ds(pl.multiple_of(g * dhalf + h * dcut, dcut), dcut)]

        def out_own(h, to):
            piece = o1_hbm.at[pl.ds(pl.multiple_of(g * dhalf + h * dcut, dcut), dcut)]
            return rcopy(piece, out_piece(z, h), ozs, ozr.at[z, h], 2 * to + y, t)

        def out_pass(c, h, to):
            piece = out_piece(c, h)
            return rcopy(piece, piece, ozs, ozr.at[c, h], 2 * to + y, t)

        def out_hand(c, h):
            piece = out_piece(c, h)
            return rcopy(piece, piece, oxs, oxr.at[c], s, t, 1 - g)

        def out_start():
            for h in range(cuts):
                @pl.when(z < levels - 1)
                def _():
                    out_own(h, z + 1).start()

                @pl.when(z > 0)
                def _():
                    out_own(h, z - 1).start()

        def out_hop(d):
            for h in range(cuts):
                @pl.when(z >= d)
                def _():
                    arrived(out_piece(z - d, h), ozr.at[z - d, h])

                    @pl.when(z < levels - 1)
                    def _():
                        out_pass(z - d, h, z + 1).start()

                    out_hand(z - d, h).start()

                @pl.when(z + d < levels)
                def _():
                    arrived(out_piece(z + d, h), ozr.at[z + d, h])

                    @pl.when(z > 0)
                    def _():
                        out_pass(z + d, h, z - 1).start()

                    out_hand(z + d, h).start()

        def two_half(e, part):
            return outs.at[1, e, pl.ds(pl.multiple_of(part * dhalf, dhalf), dhalf)]

        def two_own(e, sp):
            piece = o2_hbm.at[pl.ds(pl.multiple_of(g * dhalf, dhalf), dhalf)]
            return rcopy(piece, two_half(e, g), ns, nr.at[e], sp, t)

        def two_side():
            piece = two_half(2 + y, g)
            return rcopy(piece, piece, ns, nr.at[2 + y], side, t)

        def two_hand(e):
            piece = two_half(e, g)
            return rcopy(piece, piece, nxs, nxr.at[e], s, t, 1 - g)

        def two_start():
            two_own(2 + y, 2 * across + y).start()

        def two_near():
            arrived(two_half(2 + y, g), nr.at[2 + y])
            two_side().start()
            two_hand(2 + y).start()

        def two_far():
            arrived(two_half(2 + v, g), nr.at[2 + v])
            two_hand(2 + v).start()

        def out_drain():
            for at in range(levels):
                count = (1 + at if at < levels - 1 else 0) + (levels - at if at > 0 else 0)
                block = rows2.at[pl.ds(0, count)]

                @pl.when(z == at)
                def _():
                    arrived(block, ozs)

            arrived(rows2.at[pl.ds(0, levels - 1)], oxs)

        out_start()
        for i in range(3):
            head_copy(i, side).start()
        for a in range(1, levels):
            for j in (y, v):
                for i in range(3):
                    head_copy(i, 2 * by_distance(a) + j).start()
        for i in range(3):
            pltpu.make_async_copy(
                qkv[i].at[:, lanes(s)], heads.at[i, trows(s, reach)], hr.at[s]
            ).start()
        for i in range(3):
            pltpu.make_async_copy(
                wqkv[i].at[:, lanes(s)],
                weights.at[pl.ds(pl.multiple_of(s * wrows, wrows), wrows), pl.ds(i * head, head)],
                wr.at[s],
            ).start()
        two_own(y, side).start()
        for k in range(0, 3):
            for i in range(3):
                weight_copy(i, close(k)).start()
        local = [
            pltpu.make_async_copy(o1_hbm, outs.at[0, z], loc_sem.at[0]),
            pltpu.make_async_copy(o2_hbm, outs.at[1, y], loc_sem.at[1]),
            pltpu.make_async_copy(
                resid_hbm.at[pl.ds(pl.multiple_of(t * share, share), share)], res, loc_sem.at[2]
            ),
        ]
        for copy in local:
            copy.start()

        for copy in small:
            copy.wait()
        near = 2 * REL_CLIP
        query = lax.broadcasted_iota(jnp.int32, (tok, span), 0) // SEG
        key = lax.broadcasted_iota(jnp.int32, (tok, span), 1) // SEG
        live = (key >= query) & (key <= query + LEFT)
        for layer, rel in enumerate((rel1, rel2)):
            table = rel[pl.ds(s, 1), :]
            top = table[:, near : near + 1]
            entry = lax.broadcasted_iota(jnp.int32, (near, near + tok), 0)
            place = lax.broadcasted_iota(jnp.int32, (near, near + tok), 1)
            flip = (entry + place == near).astype(F32)
            line = jnp.dot(
                jnp.broadcast_to(table[:, :near], (8, near)), flip,
                preferred_element_type=F32, precision=lax.Precision.HIGHEST,
            )[:1]
            spot = lax.broadcasted_iota(jnp.int32, line.shape, 1)
            line = jnp.where((spot == 0) | (spot >= near), top, line)
            spread = jnp.broadcast_to(line, (tok, near + tok))
            row = lax.broadcasted_iota(jnp.int32, spread.shape, 0)
            step = 1
            while step < tok:
                moved = pltpu.roll(spread, step, 1)
                spread = jnp.where(lax.rem(row // step, 2) == 1, moved, spread)
                step *= 2
            far = jnp.broadcast_to(top, (tok, span - near))
            whole = jnp.concatenate([far, spread[:, :near]], axis=1)
            bias[layer] = jnp.where(live, whole, NEG_FILL)

        heads[1, :reach] = jnp.zeros((reach, head), BF16)
        heads[2, :reach] = jnp.zeros((reach, head), BF16)

        def attend(layer, b):
            qb = heads[0, trows(b, reach)]
            kb = heads[1, pl.ds(pl.multiple_of(b * tok, tok), span)]
            vb = heads[2, pl.ds(pl.multiple_of(b * tok, tok), span)]
            scores = lax.dot_general(
                qb, kb, (((1,), (1,)), ((), ())), preferred_element_type=F32
            ) * head ** (-0.5) + bias[layer]
            column = lax.broadcasted_iota(jnp.int32, scores.shape, 1)
            scores = jnp.where(column >= reach - b * tok, scores, NEG_FILL)
            e = jnp.exp(scores - jnp.max(scores, axis=-1, keepdims=True))
            e = (e * (1.0 / jnp.sum(e, axis=-1, keepdims=True))).astype(BF16)
            return jnp.dot(e, vb, preferred_element_type=F32).astype(BF16)

        def mix_z(layer, b):
            dst = mixed.at[layer, s, trows(lax.rem(b, 2))]
            return rcopy(
                own_mix.at[layer, b], dst, mzs.at[layer], mzr.at[layer, z], 2 * (b // 2) + y, t
            )

        def mix_y(layer, c):
            block = mixed.at[layer, 2 * c + y]
            return rcopy(block, block, mys.at[layer], myr.at[layer, c], side, t)

        def one_head(layer, order, wait_block):
            def one(i, _):
                b = order(i)
                wait_block(b)
                result = attend(layer, b)

                @pl.when(b // 2 != z)
                def _():
                    own_mix[layer, b] = result
                    mix_z(layer, b).start()

                @pl.when(b // 2 == z)
                def _():
                    mixed[layer, s, trows(lax.rem(b, 2))] = result

                    @pl.when(lax.rem(b, 2) == 1)
                    def _():
                        mix_y(layer, z).start()

                return 0

            return one

        def forward_mix(layer):
            def one(i, _):
                c = near_level(i)
                arrived(mixed.at[layer, 2 * c + y], mzr.at[layer, c])
                mix_y(layer, c).start()
                return 0

            lax.fori_loop(1, levels, one, 0)

        def two_copy(layer, b, level):
            dst = mixed.at[layer, s, trows(lax.rem(b // 2, 2))]
            return rcopy(
                own_mix.at[layer, b], dst, ms, mr,
                2 * level + lax.rem(b, 2), t,
            )

        def two_head(layer, order, wait_block):
            def one(i, _):
                b = order(i)
                wait_block(b)
                result = attend(layer, b)
                own_mix[layer, b] = result
                level = b // 2
                other = level + 1 - 2 * lax.rem(level, 2)
                mine = lax.rem(b, 2) == y

                @pl.when(jnp.logical_not(mine & (level == z)))
                def _():
                    two_copy(layer, b, level).start()

                @pl.when(jnp.logical_not(mine & (other == z)))
                def _():
                    two_copy(layer, b, other).start()

                @pl.when(mine & (level // 2 == z // 2))
                def _():
                    mixed[layer, s, trows(lax.rem(level, 2))] = result

                return 0

            return one

        def pcopy(layer, c):
            return rcopy(
                parts.at[layer, c, u], inbox.at[layer, c],
                ps.at[layer], pr.at[layer, c], s, u,
            )

        def bcopy(layer, c):
            if layer == 0:
                return rcopy(
                    joined.at[layer, c, v], branch.at[layer, y, c], bs.at[layer], br.at[layer],
                    side, t,
                )
            return rcopy(
                joined.at[layer, c, 1 - rung], branch.at[layer, rung, c],
                bs.at[layer], br.at[layer], 2 * twin + y, t,
            )

        def project_branch(layer):
            if layer == 0:
                for c in range(levels):
                    arrived(mixed.at[layer, 2 * c + v], myr.at[layer, c])
                own_block, mine, order = z, y, near_level
                hand_ready = lambda c: arrived(out_half(c, 1 - g), oxr.at[c])
            else:
                arrived(mixed.at[layer, pl.ds(0, n - 1)], mr)
                own_block, mine = y, rung
                order = lambda i: 2 * (i // 2) + lax.rem(y + i, 2)
                hand_ready = lambda e: arrived(two_half(e, 1 - g), nxr.at[e])
            local[layer].wait()

            def project(c):
                @pl.when(c != own_block)
                def _():
                    hand_ready(c)

                lhs = jnp.concatenate([mixed[layer, j] for j in range(n)], axis=1)
                part = jnp.dot(lhs, outs[layer, c], preferred_element_type=F32).astype(BF16)
                for p in range(2):
                    for q in range(2):
                        parts[layer, c, q, p] = part[p * tok + q * share : p * tok + (q + 1) * share]
                pcopy(layer, c).start()

            def join(c):
                arrived(inbox.at[layer, c], pr.at[layer, c])
                both = parts[layer, c, t].astype(F32) + inbox[layer, c].astype(F32)
                joined[layer, c] = both.astype(BF16)
                bcopy(layer, c).start()
                branch[layer, mine, c] = joined[layer, c, mine]

            def step(i, _):
                project(order(i))

                @pl.when(i > 0)
                def _():
                    join(order(i - 1))

                return 0

            lax.fori_loop(0, levels, step, 0)
            join(order(levels - 1))
            arrived(branch.at[layer, 1 - mine], br.at[layer])

            def column_block(j):
                if layer == 0:
                    return branch[layer, j % 2, j // 2]
                half = lax.rem(j // levels + 2 * z // levels, 2)
                return branch[layer, (j // 2) % 2, 2 * half + j % 2]

            values = jnp.concatenate([column_block(j) for j in range(n)], axis=1)
            return values.astype(F32)

        def branch_drain(layer):
            if layer == 0:
                arrived(own_mix.at[layer, pl.ds(0, n - 2)], mzs.at[layer])
                arrived(mixed.at[layer, pl.ds(0, levels)], mys.at[layer])
            else:
                arrived(mixed.at[layer, pl.ds(0, n - 1)], ms)
            arrived(inbox.at[layer], ps.at[layer])
            arrived(branch.at[layer, 0], bs.at[layer])

        def hand_weights(src):
            arrived(weight_half(src, g), wr.at[src])
            weight_hand(src).start()
            return 0

        def heads_ready(b):
            arrived(heads.at[:, trows(b, reach)], hr.at[b])

        out_hop(1)
        lax.fori_loop(0, n, one_head(0, lambda i: i, heads_ready), 0)
        lax.fori_loop(0, 3, lambda k, c: hand_weights(close(k)), 0)
        out_hop(2)
        forward_mix(0)
        for k in range(0, 4):
            for i in range(3):
                weight_copy(i, distant(k)).start()
        for d in range(3, levels):
            out_hop(d)
        values = project_branch(0)
        local[2].wait()
        hidden = (res[...].astype(F32) + scaled(values) * post1[...]).astype(BF16)
        res[...] = hidden
        rows2[2 * s + t] = (scaled(hidden.astype(F32)) * pre2[...]).astype(BF16)

        def piece_of(item, m):
            return rows2.at[item, :, pl.ds(pl.multiple_of(m * wide, wide), wide)]

        def row_z(c, m, to):
            block = piece_of(2 * (2 * c + y) + t, m)
            return rcopy(block, block, rzs, rzr.at[c, m], 2 * to + y, t)

        def row_y(c, m):
            block = piece_of(2 * (2 * c + y) + t, m)
            return rcopy(block, block, rys, ryr.at[c, m], side, t)

        def row_d(src, m):
            block = piece_of(2 * src + t, m)
            return rcopy(block, block, rds, rdr.at[src // 2], s, u)

        def own_rows(m, _):
            @pl.when(z < levels - 1)
            def _():
                row_z(z, m, z + 1).start()

            @pl.when(z > 0)
            def _():
                row_z(z, m, z - 1).start()

            return 0

        def own_beside(m, _):
            row_y(z, m).start()
            row_d(s, m).start()
            return 0

        lax.fori_loop(0, pieces, own_rows, 0)
        lax.fori_loop(0, pieces, own_beside, 0)
        two_start()

        lax.fori_loop(0, 4, lambda k, c: hand_weights(distant(k)), 0)
        arrived(two_half(v, g), nr.at[v])
        two_hand(v).start()

        def from_level(c, m, on, to):
            arrived(piece_of(2 * (2 * c + y) + t, m), rzr.at[c, m])

            @pl.when(on)
            def _():
                row_z(c, m, to).start()

            row_y(c, m).start()
            row_d(2 * c + y, m).start()

        def from_side(c, m):
            arrived(piece_of(2 * (2 * c + v) + t, m), ryr.at[c, m])
            row_d(2 * c + v, m).start()

        def rows_hop(d):
            def one(m, _):
                if d < levels:
                    @pl.when(z >= d)
                    def _():
                        from_level(z - d, m, z < levels - 1, z + 1)

                    @pl.when(z + d < levels)
                    def _():
                        from_level(z + d, m, z > 0, z - 1)

                if d == 1:
                    from_side(z, m)
                else:
                    @pl.when(z >= d - 1)
                    def _():
                        from_side(z - (d - 1), m)

                    @pl.when(z + d - 1 < levels)
                    def _():
                        from_side(z + (d - 1), m)

                return 0

            lax.fori_loop(0, pieces, one, 0)

        def project_rows(i, _):
            c = by_distance(i)
            arrived(rows2.at[pl.ds(4 * c, 2)], rdr.at[c])
            lhs = rows2[pl.ds(4 * c, 4)].reshape(2 * tok, width)
            both = jnp.dot(lhs, weights[...], preferred_element_type=F32).astype(BF16)
            start = pl.ds(pl.multiple_of(reach + c * 2 * tok, tok), 2 * tok)
            for i in range(3):
                heads[i, start] = both[:, i * head : (i + 1) * head]
            return 0

        def weights_here():
            arrived(weights.at[pl.ds(0, (n - 1) * hrows)], wh)
            arrived(weights.at[pl.ds(pl.multiple_of(s * wrows, wrows), wrows)], wr.at[s])

        lag = reach // tok
        top = z == levels - 1
        early = jnp.where(top, n - 2 - lag, jnp.where(z == 0, n - 2, n))
        begin = jnp.where(top, lag + 2, jnp.where(2 * z < levels, lag, 0))

        def two_order(i):
            first = lax.rem(lag + i, n - 2)
            return jnp.where(z == 0, jnp.where(i < n - 2, first, i), lax.rem(begin + i, n))

        known = jnp.where(top | (z == 0), levels - 1, levels)
        head_two = two_head(1, two_order, lambda b: None)

        for d in range(1, levels + 1):
            rows_hop(d)
            if d == 2:
                weights_here()
                lax.fori_loop(0, 2, project_rows, 0)
            if d == levels - 1:
                two_near()
                lax.fori_loop(2, known, project_rows, 0)
                lax.fori_loop(0, early, head_two, 0)
        lax.fori_loop(known, levels, project_rows, 0)
        lax.fori_loop(early, n, head_two, 0)
        two_far()
        values = project_branch(1)
        done = (res[...].astype(F32) + scaled(values) * post2[...]).astype(BF16)
        mine_rows = out_ref.at[pl.ds(pl.multiple_of(t * share, share), share)]
        mine_rows[...] = done
        final = rcopy(mine_rows, mine_rows, fs, fr, s, u)
        final.start()

        arrived(heads.at[:, pl.ds(reach, (n - 1) * tok)], hs)
        arrived(weights.at[pl.ds(0, (n - 1) * hrows)], ws)
        arrived(weights.at[pl.ds(0, (n - 1) * hrows)], wf)
        out_drain()
        arrived(rows2.at[pl.ds(0, 3)], ns)
        arrived(rows2.at[pl.ds(0, 3)], nxs)
        for layer in range(2):
            branch_drain(layer)
        for at in range(levels):
            count = (1 + at if at < levels - 1 else 0) + (levels - at if at > 0 else 0)
            block = rows2.at[pl.ds(0, count)]

            @pl.when(z == at)
            def _():
                arrived(block, rzs)

        arrived(rows2.at[pl.ds(0, levels)], rys)
        arrived(rows2.at[pl.ds(0, n)], rds)
        final.wait_send()
        other_rows = out_ref.at[pl.ds(pl.multiple_of(u * share, share), share)]
        rcopy(other_rows, other_rows, fs, fr, s, u).wait_recv()

    dma = pltpu.SemaphoreType.DMA
    scratch = [
        pltpu.VMEM((3, reach + n * tok, head), BF16),
        pltpu.VMEM((width, 3 * head), BF16),
        pltpu.VMEM((2, levels, depth, cols), BF16),
        pltpu.VMEM((share, width), BF16),
        pltpu.VMEM((2, tok, span), F32),
        pltpu.VMEM((2, n, tok, head), BF16),
        pltpu.VMEM((2, n, 2 * tok, head), BF16),
        pltpu.VMEM((2, levels, 2, 2, share, cols), BF16),
        pltpu.VMEM((2, levels, 2, share, cols), BF16),
        pltpu.VMEM((2, levels, 2, share, cols), BF16),
        pltpu.VMEM((2, 2, levels, share, cols), BF16),
        pltpu.VMEM((2 * n, share, width), BF16),
        pltpu.VMEM((n, 2 * REL_CLIP + 1), F32),
        pltpu.VMEM((n, 2 * REL_CLIP + 1), F32),
        pltpu.VMEM((1, width), F32),
        pltpu.VMEM((1, width), F32),
        pltpu.VMEM((1, width), F32),
        dma((8,)),
        dma, dma((n,)),
        dma, dma((n,)), dma, dma,
        dma((1,)), dma((1, levels)), dma((1,)), dma((1, levels)),
        dma, dma((levels, cuts)), dma, dma((levels,)),
        dma, dma, dma, dma((levels,)), dma, dma((levels,)),
        dma((2,)), dma((2, levels)), dma((2,)), dma((2,)),
        dma, dma((levels, pieces)), dma, dma((levels, pieces)), dma, dma((levels,)),
        dma, dma,
    ]
    return kernel, scratch


def by_heads(
    resid, queries_first, keys_first, values_first, rel_first, post_first, out_first, pre_second,
    query_weight, key_weight, value_weight, rel_second, post_second, out_second,
):
    n = lax.axis_size("sp")
    tok, width = resid.shape
    head = queries_first.shape[1] // rel_first.shape[0]
    kernel, scratch = build_kernel(n, tok, head, width, REACH)
    hbm = pl.BlockSpec(memory_space=pltpu.HBM)
    vmem = pl.BlockSpec(memory_space=pltpu.VMEM)
    return pl.pallas_call(
        kernel,
        out_shape=pltpu.VMEM((tok, width), BF16),
        in_specs=[hbm] * 14,
        out_specs=vmem,
        scratch_shapes=scratch,
        compiler_params=pltpu.CompilerParams(
            collective_id=0, has_side_effects=True, vmem_limit_bytes=60 * 2**20
        ),
    )(
        queries_first, keys_first, values_first, query_weight, key_weight, value_weight, resid,
        out_first, out_second, rel_first, rel_second,
        post_first[None], pre_second[None], post_second[None],
    )


def solution(mesh):
    in_specs = (
        P(("grp", "sp"), None),
        P(("grp", "sp"), "tp"),
        P(("grp", "sp"), "tp"),
        P(("grp", "sp"), "tp"),
        P("tp", None),
        P(),
        P("tp", "sp"),
        P(),
        P("sp", "tp"),
        P("sp", "tp"),
        P("sp", "tp"),
        P("tp", None),
        P(),
        P("tp", "sp"),
    )
    out_specs = P(("grp", "sp"), None)
    return jax.shard_map(shards, mesh=mesh, in_specs=in_specs, out_specs=out_specs, check_vma=False)
```
